32 devices in a mesh: dp: 4 (over y, x), kv: 4 (over z), tp: 2 (over core).
Axes of the slice: x: 2, y: 2, z: 4, core: 2. Of those that a mesh axis runs over, the one named last changes fastest.
Arguments:
- tokens: bfloat16 [192, 2048], P(('dp', 'tp'), 'kv'), may hold values from -8 to 8
- mix_gain: float32 [2048], replicated, may hold values from 0.1 to 1.9
- w_gate: bfloat16 [2048, 4096], P(None, 'kv'), may hold values from -0.125 to 0.125
- w_value: bfloat16 [2048, 4096], P(None, 'kv'), may hold values from -0.125 to 0.125
- w_maps: bfloat16 [2048, 16384], P(None, 'kv'), may hold values from -0.125 to 0.125
- w_step: bfloat16 [2048, 64], replicated, may hold values from -0.125 to 0.125
- conv_value: float32 [4, 4096], P(None, 'kv'), may hold values from -0.5 to 0.5
- conv_maps: float32 [4, 16384], P(None, 'kv'), may hold values from -0.5 to 0.5
- past_value: bfloat16 [192, 3, 4096], P(('dp', 'tp'), None, 'kv'), may hold values from -6 to 6
- past_maps: bfloat16 [192, 3, 16384], P(('dp', 'tp'), None, 'kv'), may hold values from -6 to 6
- step_bias: float32 [64], P('kv'), may hold values from -3 to 0
- decay_log: float32 [64], P('kv'), may hold values from 0 to 2.77
- skip_gain: float32 [64], P('kv'), may hold values from 0.1 to 1.9
- head_gain: float32 [4096], P('kv'), may hold values from 0.1 to 1.9
- state: float32 [192, 64, 64, 128], P(('dp', 'tp'), 'kv'), may hold values from -2 to 2
- w_out: bfloat16 [4096, 2048], P('kv'), may hold values from -0.125 to 0.125
- mlp_gain: float32 [2048], replicated, may hold values from 0.1 to 1.9
- w_up: bfloat16 [2048, 8192], P(None, 'kv'), may hold values from -0.125 to 0.125
- w_down: bfloat16 [8192, 2048], P('kv'), may hold values from -0.09375 to 0.09375
Outputs:
- layer_out: bfloat16 [192, 2048], P(('dp', 'tp'), 'kv')
- state_next: float32 [192, 64, 64, 128], P(('dp', 'tp'), 'kv')
- value_tail: bfloat16 [192, 3, 4096], P(('dp', 'tp'), None, 'kv')
- maps_tail: bfloat16 [192, 3, 16384], P(('dp', 'tp'), None, 'kv')
The draws below stay inside these ranges and needn't reach their ends.
All inputs are finite; a program needn't handle non-finite values.
Results may differ from the reference program's by a relative error of at most 0.0081.
Values may be sent and summed in bfloat16 or wider, within the bound.
No kernel may reach another device: no remote copies, remote signals or barrier semaphores. Data moves between devices by JAX's collectives and lax.ppermute only.
A program may use at most 128 MiB of HBM per device.

```python
import jax
import jax.numpy as jnp
from jax import lax

D = 2048
HEADS = 64
HEAD_DIM = 64
STATE = 128
GROUPS = 64
KERNEL = 4
FF = 8192
INNER = 4096
MAPS = 16384
BATCH = 192


def draw_tokens(key, part):
    streams = jax.random.split(jax.random.fold_in(key, 17), 4)
    columns = jnp.arange(D, dtype=jnp.float32)
    spread = jnp.exp(jax.random.uniform(streams[0], (D,), jnp.float32) * jnp.log(10.0))
    col_scale = spread * (1.0 + 3.0 * columns / D)
    col_scale = col_scale / jnp.sqrt(jnp.mean(col_scale * col_scale))
    noise_part = jax.random.normal(streams[1], (BATCH, D), jnp.float32)
    row_scale = jnp.exp(jax.random.uniform(streams[3], (BATCH, 1), jnp.float32, -0.35, 0.35))
    return jnp.clip(noise_part * col_scale[None, :] * row_scale, -8.0, 8.0).astype(jnp.bfloat16)


def with_spikes(result, stream_key, source, target, shards_of, factor):
    def block_of(position):
        return (jnp.arange(result.shape[position]) // (result.shape[position] // shards_of)).reshape((-1,) + (1,) * (result.ndim - 1 - position))

    near = jax.random.permutation(stream_key, shards_of)[block_of(target)]
    far = (block_of(target) + shards_of // 2) % shards_of
    return jnp.where((block_of(source) == near) | (block_of(source) == far), factor * result, result)


def block_levels(own_key, extent, cuts, least, largest):
    def one(position, shards_of):
        heights = jax.random.uniform(jax.random.fold_in(jax.random.fold_in(own_key, 6), position), (shards_of,), jnp.float32, least / len(cuts), largest / len(cuts))
        return jnp.repeat(jnp.exp(heights), extent[position] // shards_of).reshape((-1,) + (1,) * (len(extent) - position - 1))

    level = one(*cuts[0])
    for cut in cuts[1:]:
        level = level * one(*cut)
    return level


def noise(own_key, shape, scale, bound, cuts=(), kind=jnp.bfloat16):
    entries = jax.random.normal(own_key, shape, jnp.float32) * scale
    if len(cuts) > 0:
        entries = block_levels(own_key, shape, cuts, -0.22, 0.18) * entries
    return jnp.clip(entries, min=-bound, max=bound).astype(kind)


def heavy_noise(own_key, shape, deviation, limit, cuts, heavy, kind=jnp.bfloat16):
    entries = deviation * jax.random.normal(own_key, shape, jnp.float32)
    if cuts:
        entries = entries * block_levels(own_key, shape, cuts, -0.22, 0.18)
    return jnp.clip(with_spikes(entries, jax.random.fold_in(own_key, 3), *heavy), -limit, limit).astype(kind)


def setup_inputs(seed: int = 0) -> dict:
    streams_of = jax.random.split(jax.random.key(seed), 20)
    return {
        "tokens": draw_tokens(jax.random.fold_in(streams_of[19], 71), 0),
        "mix_gain": jnp.clip(1.0 + 0.18 * jax.random.normal(streams_of[1], (D,), jnp.float32), 0.1, 1.9),
        "w_gate": noise(streams_of[2], (D, INNER), D ** -0.5, 0.125, ((1, 4),)),
        "w_value": noise(streams_of[3], (D, INNER), D ** -0.5, 0.125, ((1, 4),)),
        "w_maps": noise(streams_of[4], (D, MAPS), D ** -0.5, 0.125, ((1, 4),)),
        "w_step": noise(streams_of[5], (D, HEADS), D ** -0.5, 0.125),
        "conv_value": jnp.clip(jax.random.uniform(streams_of[6], (KERNEL, INNER), jnp.float32, -0.5, 0.5) * block_levels(streams_of[6], (KERNEL, INNER), ((1, 4),), -0.4, 0.0), -0.5, 0.5),
        "conv_maps": jnp.clip(jax.random.uniform(streams_of[7], (KERNEL, MAPS), jnp.float32, -0.5, 0.5) * block_levels(streams_of[7], (KERNEL, MAPS), ((1, 4),), -0.4, 0.0), -0.5, 0.5),
        "past_value": noise(streams_of[8], (BATCH, KERNEL - 1, INNER), 1.0, 6.0, ((0, 8), (2, 4))),
        "past_maps": noise(streams_of[9], (BATCH, KERNEL - 1, MAPS), 1.0, 6.0, ((0, 8), (2, 4))),
        "step_bias": jnp.clip(-3.0 + 3.0 * jax.random.uniform(streams_of[10], (HEADS,), jnp.float32) ** block_levels(streams_of[10], (HEADS,), ((0, 4),), -0.2, 0.2), -3.0, 0.0),
        "decay_log": jnp.clip(2.77 * jax.random.uniform(streams_of[11], (HEADS,), jnp.float32) ** block_levels(streams_of[11], (HEADS,), ((0, 4),), -0.2, 0.2), 0.0, 2.77),
        "skip_gain": jnp.clip(1.0 + 0.18 * jax.random.normal(streams_of[12], (HEADS,), jnp.float32), 0.1, 1.9),
        "head_gain": jnp.clip(1.0 + 0.18 * jax.random.normal(streams_of[13], (INNER,), jnp.float32), 0.1, 1.9),
        "state": noise(streams_of[14], (BATCH, HEADS, HEAD_DIM, STATE), 0.3, 2.0, ((0, 8), (1, 4)), jnp.float32),
        "w_out": heavy_noise(streams_of[15], (INNER, D), INNER ** -0.5, 0.125, ((0, 4),), (0, 1, 4, 2.0)),
        "mlp_gain": jnp.clip(1.0 + 0.18 * jax.random.normal(streams_of[16], (D,), jnp.float32), 0.1, 1.9),
        "w_up": noise(streams_of[17], (D, FF), D ** -0.5, 0.125, ((1, 4),)),
        "w_down": heavy_noise(streams_of[18], (FF, D), FF ** -0.5, 0.09375, ((0, 4),), (0, 1, 4, 2.0)),
    }


NORM_EPS = 1e-05

def rms_rows(matrix, gain_vec):
    widened = matrix.astype(jnp.float32)
    inv_scale = lax.rsqrt(lax.optimization_barrier(jnp.mean(widened * widened, axis=-1, keepdims=True)) + NORM_EPS)
    return (widened * inv_scale * gain_vec).astype(jnp.bfloat16)

def short_conv(past_rows, newest, kernel):
    window = jnp.concatenate([past_rows, newest[:, None, :]], axis=1)
    summed = lax.optimization_barrier(jnp.sum(window.astype(jnp.float32) * kernel[None], axis=1))
    return (jax.nn.silu(summed), window[:, 1:, :])

def reference(tokens, mix_gain, w_gate, w_value, w_maps, w_step, conv_value, conv_maps, past_value, past_maps, step_bias, decay_log, skip_gain, head_gain, state, w_out, mlp_gain, w_up, w_down):
    normed = rms_rows(tokens, mix_gain)
    gate_pre = jnp.dot(normed, w_gate, preferred_element_type=jnp.float32)
    step_pre = jnp.dot(normed, w_step, preferred_element_type=jnp.float32)
    value_new = jnp.dot(normed, w_value, preferred_element_type=jnp.float32).astype(jnp.bfloat16)
    maps_new = jnp.dot(normed, w_maps, preferred_element_type=jnp.float32).astype(jnp.bfloat16)
    value_act, value_tail = short_conv(past_value, value_new, conv_value)
    maps_act, maps_tail = short_conv(past_maps, maps_new, conv_maps)
    rounded = lax.optimization_barrier(maps_act.astype(jnp.bfloat16))
    grouped = rounded.astype(jnp.float32).reshape(BATCH, GROUPS, 2, STATE)
    per_group = HEADS // GROUPS
    in_map = jnp.repeat(grouped[:, :, 0], per_group, axis=1)
    out_map = jnp.repeat(grouped[:, :, 1], per_group, axis=1)
    head_values = value_act.reshape(BATCH, HEADS, HEAD_DIM)
    step_size = jax.nn.softplus(step_pre + step_bias)
    decay_rate = jnp.exp(-step_size * jnp.exp(decay_log))
    written = (step_size[:, :, None] * head_values)[:, :, :, None] * in_map[:, :, None, :]
    state_next = decay_rate[:, :, None, None] * state + written
    read_out = lax.optimization_barrier(jnp.sum(state_next * out_map[:, :, None, :], axis=-1)) + skip_gain[None, :, None] * head_values
    gated_heads = read_out * jax.nn.silu(gate_pre.reshape(BATCH, HEADS, HEAD_DIM))
    inv_scale = lax.rsqrt(lax.optimization_barrier(jnp.mean(gated_heads * gated_heads, axis=-1, keepdims=True)) + NORM_EPS)
    heads_out = (gated_heads * inv_scale * head_gain.reshape(HEADS, HEAD_DIM)).reshape(BATCH, INNER)
    heads_out = heads_out.astype(jnp.bfloat16)
    mixer_out = jnp.dot(heads_out, w_out, preferred_element_type=jnp.float32)
    hidden = lax.optimization_barrier((tokens.astype(jnp.float32) + mixer_out).astype(jnp.bfloat16))
    normed_mlp = rms_rows(hidden, mlp_gain)
    squared = jnp.square(jax.nn.relu(jnp.dot(normed_mlp, w_up, preferred_element_type=jnp.float32)))
    squared = squared.astype(jnp.bfloat16)
    layer_out = hidden.astype(jnp.float32) + jnp.dot(squared, w_down, preferred_element_type=jnp.float32)
    return (layer_out.astype(jnp.bfloat16), state_next, value_tail, maps_tail)
```

```python
import functools

import jax
import jax.numpy as jnp
from jax import lax
from jax.sharding import PartitionSpec as P

HEAD_DIM = 64
STATE = 128


NORM_EPS = 1e-05


def rms_rows(matrix, gain_vec):
    widened = matrix.astype(jnp.float32)
    inv_scale = lax.rsqrt(jnp.mean(widened * widened, axis=-1, keepdims=True) + NORM_EPS)
    return (widened * inv_scale * gain_vec).astype(jnp.bfloat16)


def short_conv(past_rows, newest, kernel):
    window = jnp.concatenate([past_rows, newest[:, None, :]], axis=1)
    summed = jnp.sum(window.astype(jnp.float32) * kernel[None], axis=1)
    return (jax.nn.silu(summed), window[:, 1:, :])


def shifted(block, axis_name, size, step):
    return lax.ppermute(block, axis_name, [(i, (i + step) % size) for i in range(size)])


def gather_columns(block, axis_name, size):
    me = lax.axis_index(axis_name)
    width = block.shape[1]
    whole = jnp.zeros((block.shape[0], width * size), block.dtype)
    pieces = [block] + [shifted(block, axis_name, size, step) for step in range(1, size)]
    for step, piece in enumerate(pieces):
        source = lax.rem(me + size - step, size)
        whole = lax.dynamic_update_slice_in_dim(whole, piece, source * width, 1)
    return whole


def scatter_sum(partial, axis_name, size):
    me = lax.axis_index(axis_name)
    width = partial.shape[1] // size
    rounded = partial.astype(jnp.bfloat16)
    total = lax.dynamic_slice_in_dim(partial, me * width, width, 1)
    for step in range(1, size):
        target = lax.rem(me + step, size)
        piece = lax.dynamic_slice_in_dim(rounded, target * width, width, 1)
        total = total + shifted(piece, axis_name, size, step).astype(jnp.float32)
    return total


def few_peers(size):
    return size <= 8


def local(
    size,
    tokens,
    mix_gain,
    w_gate,
    w_value,
    w_maps,
    w_step,
    conv_value,
    conv_maps,
    past_value,
    past_maps,
    step_bias,
    decay_log,
    skip_gain,
    head_gain,
    state,
    w_out,
    mlp_gain,
    w_up,
    w_down,
):
    if few_peers(size):
        whole_rows = gather_columns(tokens, "kv", size)
    else:
        whole_rows = lax.all_gather(tokens, "kv", axis=1, tiled=True)
    batch_rows = whole_rows.shape[0]
    heads_here = state.shape[1]
    head_start = lax.axis_index("kv") * heads_here
    normed = rms_rows(whole_rows, mix_gain)
    gate_pre = jnp.dot(normed, w_gate, preferred_element_type=jnp.float32)
    step_cols = lax.dynamic_slice_in_dim(w_step, head_start, heads_here, 1)
    step_pre = jnp.dot(normed, step_cols, preferred_element_type=jnp.float32)
    value_new = jnp.dot(normed, w_value, preferred_element_type=jnp.float32).astype(jnp.bfloat16)
    maps_new = jnp.dot(normed, w_maps, preferred_element_type=jnp.float32).astype(jnp.bfloat16)
    value_act, value_tail = short_conv(past_value, value_new, conv_value)
    maps_act, maps_tail = short_conv(past_maps, maps_new, conv_maps)
    maps_act = lax.optimization_barrier(maps_act.astype(jnp.bfloat16))
    grouped = maps_act.astype(jnp.float32).reshape(batch_rows, -1, 2, STATE)
    per_group = heads_here // grouped.shape[1]
    in_map = jnp.repeat(grouped[:, :, 0], per_group, axis=1)
    out_map = jnp.repeat(grouped[:, :, 1], per_group, axis=1)
    head_values = value_act.reshape(batch_rows, heads_here, HEAD_DIM)
    step_size = jax.nn.softplus(step_pre + step_bias)
    decay_rate = jnp.exp(-step_size * jnp.exp(decay_log))
    written = (step_size[:, :, None] * head_values)[:, :, :, None] * in_map[:, :, None, :]
    state_next = decay_rate[:, :, None, None] * state + written
    read_out = (
        jnp.sum(state_next * out_map[:, :, None, :], axis=-1)
        + skip_gain[None, :, None] * head_values
    )
    gated_heads = read_out * jax.nn.silu(gate_pre.reshape(batch_rows, heads_here, HEAD_DIM))
    inv_scale = lax.rsqrt(jnp.mean(gated_heads * gated_heads, axis=-1, keepdims=True) + NORM_EPS)
    heads_out = gated_heads * inv_scale * head_gain.reshape(heads_here, HEAD_DIM)
    heads_out = heads_out.reshape(batch_rows, heads_here * HEAD_DIM).astype(jnp.bfloat16)
    partial_value = jnp.dot(heads_out, w_out, preferred_element_type=jnp.float32)
    if few_peers(size):
        own_part = scatter_sum(partial_value, "kv", size)
    else:
        own_part = lax.psum_scatter(partial_value, "kv", scatter_dimension=1, tiled=True)
    own_hidden = lax.optimization_barrier(
        (tokens.astype(jnp.float32) + own_part).astype(jnp.bfloat16)
    )
    if few_peers(size):
        hidden = gather_columns(own_hidden, "kv", size)
    else:
        hidden = lax.all_gather(own_hidden, "kv", axis=1, tiled=True)
    normed_mlp = rms_rows(hidden, mlp_gain)
    squared = jnp.square(jax.nn.relu(jnp.dot(normed_mlp, w_up, preferred_element_type=jnp.float32)))
    squared = squared.astype(jnp.bfloat16)
    partial_mlp = jnp.dot(squared, w_down, preferred_element_type=jnp.float32)
    if few_peers(size):
        mlp_part = scatter_sum(partial_mlp, "kv", size)
    else:
        mlp_part = lax.psum_scatter(partial_mlp, "kv", scatter_dimension=1, tiled=True)
    layer_out = (own_hidden.astype(jnp.float32) + mlp_part).astype(jnp.bfloat16)
    return (layer_out, state_next, value_tail, maps_tail)


def solution(mesh):
    in_specs = (
        P(("dp", "tp"), "kv"),
        P(),
        P(None, "kv"),
        P(None, "kv"),
        P(None, "kv"),
        P(),
        P(None, "kv"),
        P(None, "kv"),
        P(("dp", "tp"), None, "kv"),
        P(("dp", "tp"), None, "kv"),
        P("kv"),
        P("kv"),
        P("kv"),
        P("kv"),
        P(("dp", "tp"), "kv", None, None),
        P("kv", None),
        P(),
        P(None, "kv"),
        P("kv", None),
    )
    out_specs = (
        P(("dp", "tp"), "kv"),
        P(("dp", "tp"), "kv", None, None),
        P(("dp", "tp"), None, "kv"),
        P(("dp", "tp"), None, "kv"),
    )
    step = functools.partial(local, mesh.shape["kv"])
    return jax.shard_map(step, mesh=mesh, in_specs=in_specs, out_specs=out_specs, check_vma=False)
```

```python
import functools

import jax
import jax.numpy as jnp
from jax import lax
from jax.experimental import pallas as pl
from jax.experimental.pallas import tpu as pltpu
from jax.sharding import PartitionSpec as P

HEAD_DIM = 64
STATE = 128
LANES = 128
TILE = 512


NORM_EPS = 1e-05

VMEM = pl.BlockSpec(memory_space=pltpu.VMEM)
SMEM = pl.BlockSpec(memory_space=pltpu.SMEM)
HBM = pl.BlockSpec(memory_space=pltpu.HBM)


def rms_rows(matrix, gain_vec):
    widened = matrix.astype(jnp.float32)
    inv_scale = lax.rsqrt(jnp.mean(widened * widened, axis=-1, keepdims=True) + NORM_EPS)
    return (widened * inv_scale * gain_vec).astype(jnp.bfloat16)


def short_conv(past_rows, newest, kernel):
    window = jnp.concatenate([past_rows, newest[:, None, :]], axis=1)
    summed = jnp.sum(window.astype(jnp.float32) * kernel[None], axis=1)
    return (jax.nn.silu(summed), window[:, 1:, :])


def local_many(
    tokens,
    mix_gain,
    w_gate,
    w_value,
    w_maps,
    w_step,
    conv_value,
    conv_maps,
    past_value,
    past_maps,
    step_bias,
    decay_log,
    skip_gain,
    head_gain,
    state,
    w_out,
    mlp_gain,
    w_up,
    w_down,
):
    whole_rows = lax.all_gather(tokens, "kv", axis=1, tiled=True)
    batch_rows = whole_rows.shape[0]
    heads_here = state.shape[1]
    head_start = lax.axis_index("kv") * heads_here
    normed = rms_rows(whole_rows, mix_gain)
    gate_pre = jnp.dot(normed, w_gate, preferred_element_type=jnp.float32)
    step_cols = lax.dynamic_slice_in_dim(w_step, head_start, heads_here, 1)
    step_pre = jnp.dot(normed, step_cols, preferred_element_type=jnp.float32)
    value_new = jnp.dot(normed, w_value, preferred_element_type=jnp.float32).astype(jnp.bfloat16)
    maps_new = jnp.dot(normed, w_maps, preferred_element_type=jnp.float32).astype(jnp.bfloat16)
    value_act, value_tail = short_conv(past_value, value_new, conv_value)
    maps_act, maps_tail = short_conv(past_maps, maps_new, conv_maps)
    maps_act = lax.optimization_barrier(maps_act.astype(jnp.bfloat16))
    grouped = maps_act.astype(jnp.float32).reshape(batch_rows, -1, 2, STATE)
    per_group = heads_here // grouped.shape[1]
    in_map = jnp.repeat(grouped[:, :, 0], per_group, axis=1)
    out_map = jnp.repeat(grouped[:, :, 1], per_group, axis=1)
    head_values = value_act.reshape(batch_rows, heads_here, HEAD_DIM)
    step_size = jax.nn.softplus(step_pre + step_bias)
    decay_rate = jnp.exp(-step_size * jnp.exp(decay_log))
    written = (step_size[:, :, None] * head_values)[:, :, :, None] * in_map[:, :, None, :]
    state_next = decay_rate[:, :, None, None] * state + written
    read_out = (
        jnp.sum(state_next * out_map[:, :, None, :], axis=-1)
        + skip_gain[None, :, None] * head_values
    )
    gated_heads = read_out * jax.nn.silu(gate_pre.reshape(batch_rows, heads_here, HEAD_DIM))
    inv_scale = lax.rsqrt(jnp.mean(gated_heads * gated_heads, axis=-1, keepdims=True) + NORM_EPS)
    heads_out = gated_heads * inv_scale * head_gain.reshape(heads_here, HEAD_DIM)
    heads_out = heads_out.reshape(batch_rows, heads_here * HEAD_DIM).astype(jnp.bfloat16)
    partial_value = jnp.dot(heads_out, w_out, preferred_element_type=jnp.float32)
    own_part = lax.psum_scatter(partial_value, "kv", scatter_dimension=1, tiled=True)
    own_hidden = lax.optimization_barrier(
        (tokens.astype(jnp.float32) + own_part).astype(jnp.bfloat16)
    )
    hidden = lax.all_gather(own_hidden, "kv", axis=1, tiled=True)
    normed_mlp = rms_rows(hidden, mlp_gain)
    squared = jnp.square(jax.nn.relu(jnp.dot(normed_mlp, w_up, preferred_element_type=jnp.float32)))
    squared = squared.astype(jnp.bfloat16)
    partial_mlp = jnp.dot(squared, w_down, preferred_element_type=jnp.float32)
    mlp_part = lax.psum_scatter(partial_mlp, "kv", scatter_dimension=1, tiled=True)
    layer_out = (own_hidden.astype(jnp.float32) + mlp_part).astype(jnp.bfloat16)
    return (layer_out, state_next, value_tail, maps_tail)


def shifted(block, size, step):
    return lax.ppermute(block, "kv", [(i, (i + step) % size) for i in range(size)])


def in_hbm(array):
    return pltpu.with_memory_space_constraint(array, pltpu.HBM)


def cost(flops, moved):
    return pl.CostEstimate(flops=int(flops), bytes_accessed=int(moved), transcendentals=0)


def silu(x):
    return x / (1.0 + jnp.exp(-x))


def fetch_kernel(parts, *refs):
    count = (len(refs) - 1) // 2
    sources, targets, sems = refs[-1 - 2 * count : -1 - count], refs[-1 - count : -1], refs[-1]
    copies = []
    for which in range(count):
        rows = sources[which].shape[0] // parts
        for part in range(parts):
            block = pl.ds(part * rows, rows)
            copies.append(
                pltpu.make_async_copy(
                    sources[which].at[block], targets[which].at[block], sems.at[which * parts + part]
                )
            )
    for copy in copies:
        copy.start()
    for copy in copies:
        copy.wait()


def fetch(after, arrays, name, flops, parts=4):
    moved = sum(a.size * a.dtype.itemsize for a in arrays)
    first = [] if after is None else [after]
    return pl.pallas_call(
        functools.partial(fetch_kernel, parts),
        out_shape=[pltpu.VMEM(a.shape, a.dtype) for a in arrays],
        in_specs=[pl.BlockSpec(memory_space=pl.ANY)] * len(first) + [HBM] * len(arrays),
        out_specs=[VMEM] * len(arrays),
        scratch_shapes=[pltpu.SemaphoreType.DMA((parts * len(arrays),))],
        compiler_params=pltpu.CompilerParams(vmem_limit_bytes=1 << 20),
        cost_estimate=cost(flops, 2 * moved),
        name=name,
    )(*first, *[in_hbm(a) for a in arrays])


def mixer_kernel(size, *refs):
    me_ref, bias_ref, dlog_ref, skip_ref = refs[:4]
    chunks = refs[4 : 4 + size]
    (gain, wstep, conv_v, conv_m, hgain, wmaps, past_v, past_m, wvalue, wgate, state, wout) = refs[
        4 + size : 16 + size
    ]
    (part_o, x_o, state_o, dec_o, in_o, u_o, vtail, mtail) = refs[16 + size : 24 + size]
    (wvalue_s, wgate_s, wout_s, pastv_s, pastm_s, newv_s, newm_s, out_s, value_s, gate_s, heads_s, sems, ssems) = refs[
        24 + size :
    ]
    rows, width = chunks[0].shape
    me = me_ref[0]
    heads = state.shape[1]
    pairs = heads // 2

    def state_copy(pair):
        both = pl.ds(2 * pair, 2)
        return pltpu.make_async_copy(state.at[:, both], state_o.at[:, both], ssems.at[pair])

    loads = [
        pltpu.make_async_copy(past_m, pastm_s, sems.at[0]),
        pltpu.make_async_copy(past_v, pastv_s, sems.at[1]),
        pltpu.make_async_copy(wvalue, wvalue_s, sems.at[2]),
        pltpu.make_async_copy(wgate, wgate_s, sems.at[3]),
    ]
    for copy in loads:
        copy.start()
    for pair in range(pairs):
        state_copy(pair).start()
    load_out = pltpu.make_async_copy(wout, wout_s, sems.at[4])
    load_out.start()

    for step in range(size):
        source = lax.rem(me + size - step, size)
        x_o[:, pl.ds(pl.multiple_of(source * width, width), width)] = chunks[step][...]
    x = x_o[...].astype(jnp.float32)
    inv = lax.rsqrt(jnp.mean(x * x, axis=-1, keepdims=True) + NORM_EPS)
    normed = (x * inv * gain[...]).astype(jnp.bfloat16)

    step_pre = lax.dot_general(
        normed, wstep[...], (((1,), (1,)), ((), ())), preferred_element_type=jnp.float32
    )

    def conv(past, new, taps, block):
        total = new.astype(jnp.float32) * taps[3:4, block]
        for t in range(3):
            total = total + past[t, :, block].astype(jnp.float32) * taps[t : t + 1, block]
        return silu(total)

    loads[0].wait()
    tails = [pltpu.make_async_copy(pastm_s.at[pl.ds(1, 2)], mtail.at[pl.ds(0, 2)], sems.at[5])]
    tails[0].start()
    for tile in range(wmaps.shape[1] // TILE):
        block = pl.ds(tile * TILE, TILE)
        new = jnp.dot(normed, wmaps[:, block], preferred_element_type=jnp.float32).astype(jnp.bfloat16)
        newm_s[:, block] = new
        act = conv(pastm_s, new, conv_m, block).astype(jnp.bfloat16).astype(jnp.float32)
        for half in range(TILE // (2 * STATE)):
            head = tile * (TILE // (2 * STATE)) + half
            base = half * 2 * STATE
            in_o[:, pl.ds(head * STATE, STATE)] = act[:, base : base + STATE]
            out_s[:, pl.ds(head * STATE, STATE)] = act[:, base + STATE : base + 2 * STATE]
    tails.append(pltpu.make_async_copy(newm_s, mtail.at[2], sems.at[6]))
    tails[1].start()

    loads[1].wait()
    tails.append(pltpu.make_async_copy(pastv_s.at[pl.ds(1, 2)], vtail.at[pl.ds(0, 2)], sems.at[7]))
    tails[2].start()
    loads[2].wait()
    for tile in range(wvalue_s.shape[1] // TILE):
        block = pl.ds(tile * TILE, TILE)
        new = jnp.dot(normed, wvalue_s[:, block], preferred_element_type=jnp.float32).astype(jnp.bfloat16)
        newv_s[:, block] = new
        value_s[:, block] = conv(pastv_s, new, conv_v, block)
    tails.append(pltpu.make_async_copy(newv_s, vtail.at[2], sems.at[8]))
    tails[3].start()
    loads[3].wait()
    for tile in range(wgate_s.shape[1] // TILE):
        block = pl.ds(tile * TILE, TILE)
        gate_s[:, block] = silu(jnp.dot(normed, wgate_s[:, block], preferred_element_type=jnp.float32))

    lane = lax.broadcasted_iota(jnp.int32, (HEAD_DIM, LANES), 1)
    low = lax.broadcasted_iota(jnp.int32, (rows, LANES), 1) < HEAD_DIM
    step_lane = lax.broadcasted_iota(jnp.int32, step_pre.shape, 1)

    def pair_body(pair, carry):
        state_copy(pair).wait()
        gathered, decays, sizes, meets = [], [], [], []
        for which in range(2):
            head = 2 * pair + which
            wide = pl.ds(pl.multiple_of(head * STATE, STATE), STATE)
            column = jnp.sum(
                jnp.where(step_lane == me * heads + head, step_pre, 0.0), axis=1, keepdims=True
            )
            pre = jnp.broadcast_to(column, (rows, LANES)) + bias_ref[head]
            size_h = jnp.maximum(pre, 0.0) + jnp.log1p(jnp.exp(-jnp.abs(pre)))
            rate = jnp.exp(jnp.full((rows, LANES), dlog_ref[head]))
            decay = jnp.exp(-size_h * rate)
            dec_o[:, wide] = decay
            out_h = out_s[:, wide]
            meets.append(jnp.sum(in_o[:, wide] * out_h, axis=1, keepdims=True))
            decays.append(decay)
            sizes.append(size_h)
            total = jnp.zeros((HEAD_DIM, LANES), jnp.float32)
            for row in range(rows):
                dots = jnp.sum(state_o[row, head] * out_h[row : row + 1], axis=1, keepdims=True)
                total = jnp.where(lane == row, dots, total)
            gathered.append(total)
        carried = jnp.transpose(jnp.concatenate(gathered, axis=0))[:rows]
        block = pl.ds(pl.multiple_of(pair * LANES, LANES), LANES)
        value = value_s[:, block]
        written = jnp.where(low, sizes[0], sizes[1]) * value
        u_o[block, :] = jnp.transpose(written)
        read = jnp.where(low, decays[0], decays[1]) * carried
        read = read + jnp.where(low, meets[0], meets[1]) * written
        read = read + jnp.where(low, skip_ref[2 * pair], skip_ref[2 * pair + 1]) * value
        gated = read * gate_s[:, block]
        square = gated * gated
        first = jnp.sum(jnp.where(low, square, 0.0), axis=1, keepdims=True)
        second = jnp.sum(jnp.where(low, 0.0, square), axis=1, keepdims=True)
        scale = lax.rsqrt(jnp.where(low, first, second) * (1.0 / HEAD_DIM) + NORM_EPS)
        heads_s[:, block] = (gated * scale * hgain[:, block]).astype(jnp.bfloat16)
        return carry

    lax.fori_loop(0, pairs, pair_body, 0)

    load_out.wait()
    merged = heads_s[...]
    for tile in range(wout_s.shape[1] // TILE):
        block = pl.ds(tile * TILE, TILE)
        part_o[:, block] = jnp.dot(merged, wout_s[:, block], preferred_element_type=jnp.float32).astype(
            jnp.bfloat16
        )
    for copy in tails:
        copy.wait()


def write_kernel(state_ref, dec_ref, in_ref, u_ref, next_ref):
    rows = state_ref.shape[0]
    pair = pl.program_id(0)
    for which in range(2):
        head = 2 * pair + which
        wide = pl.ds(pl.multiple_of(head * STATE, STATE), STATE)
        column = u_ref[pl.ds(pl.multiple_of(head * HEAD_DIM, HEAD_DIM), HEAD_DIM), :]
        decay, in_map = dec_ref[:, wide], in_ref[:, wide]
        for row in range(rows):
            next_ref[row, which] = (
                state_ref[row, head] * decay[row : row + 1]
                + column[:, row : row + 1] * in_map[row : row + 1]
            )


def mlp_kernel(size, *refs):
    me_ref, x_ref = refs[:2]
    parts = refs[2 : 2 + size]
    gain, wup, wdown = refs[2 + size : 5 + size]
    base_o = refs[5 + size]
    pieces = refs[6 + size : 5 + 2 * size]
    hidden_s, total_s = refs[5 + 2 * size :]
    width = base_o.shape[1]
    me = me_ref[0]
    total = x_ref[...].astype(jnp.float32)
    for part in parts:
        total = total + part[...].astype(jnp.float32)
    hidden = total.astype(jnp.bfloat16)
    hidden_s[...] = hidden.astype(jnp.float32)
    wide = hidden_s[...]
    inv = lax.rsqrt(jnp.mean(wide * wide, axis=-1, keepdims=True) + NORM_EPS)
    normed = (wide * inv * gain[...]).astype(jnp.bfloat16)
    out = None
    for tile in range(wup.shape[1] // TILE):
        block = pl.ds(tile * TILE, TILE)
        up = jnp.maximum(jnp.dot(normed, wup[:, block], preferred_element_type=jnp.float32), 0.0)
        squared = (up * up).astype(jnp.bfloat16)
        down = jnp.dot(squared, wdown[block, :], preferred_element_type=jnp.float32)
        out = down if out is None else out + down
    total_s[...] = out
    own = pl.ds(pl.multiple_of(me * width, width), width)
    base_o[...] = hidden_s[:, own] + total_s[:, own]
    for step in range(1, size):
        target = lax.rem(me + step, size)
        block = pl.ds(pl.multiple_of(target * width, width), width)
        pieces[step - 1][...] = total_s[:, block].astype(jnp.bfloat16)


def local_few(
    size,
    tokens,
    mix_gain,
    w_gate,
    w_value,
    w_maps,
    w_step,
    conv_value,
    conv_maps,
    past_value,
    past_maps,
    step_bias,
    decay_log,
    skip_gain,
    head_gain,
    state,
    w_out,
    mlp_gain,
    w_up,
    w_down,
):
    f32, bf16 = jnp.float32, jnp.bfloat16
    rows, width = tokens.shape
    model = width * size
    heads = state.shape[1]
    inner, maps = w_value.shape[1], w_maps.shape[1]
    me = lax.axis_index("kv").astype(jnp.int32).reshape(1)

    chunks = [tokens] + [shifted(tokens, size, step) for step in range(1, size)]
    (maps_near,) = fetch(None, [w_maps], "fetch_maps", 1e6)
    part, whole, held, decay, in_map, written, value_tail, maps_tail = pl.pallas_call(
        functools.partial(mixer_kernel, size),
        out_shape=[
            pltpu.VMEM((rows, model), bf16),
            pltpu.VMEM((rows, model), bf16),
            pltpu.VMEM(state.shape, f32),
            pltpu.VMEM((rows, heads * STATE), f32),
            pltpu.VMEM((rows, heads * STATE), f32),
            pltpu.VMEM((inner, rows), f32),
            jax.ShapeDtypeStruct((3, rows, inner), bf16),
            jax.ShapeDtypeStruct((3, rows, maps), bf16),
        ],
        in_specs=[SMEM] * 4 + [VMEM] * (size + 6) + [HBM] * 6,
        out_specs=[VMEM] * 6 + [HBM] * 2,
        scratch_shapes=[
            pltpu.VMEM(w_value.shape, bf16),
            pltpu.VMEM(w_gate.shape, bf16),
            pltpu.VMEM(w_out.shape, bf16),
            pltpu.VMEM((3, rows, inner), bf16),
            pltpu.VMEM((3, rows, maps), bf16),
            pltpu.VMEM((rows, inner), bf16),
            pltpu.VMEM((rows, maps), bf16),
            pltpu.VMEM((rows, heads * STATE), f32),
            pltpu.VMEM((rows, inner), f32),
            pltpu.VMEM((rows, inner), f32),
            pltpu.VMEM((rows, inner), bf16),
            pltpu.SemaphoreType.DMA((9,)),
            pltpu.SemaphoreType.DMA((heads // 2,)),
        ],
        compiler_params=pltpu.CompilerParams(vmem_limit_bytes=20 << 20),
        cost_estimate=cost(2 * rows * model * (2 * inner + maps), 40e6),
        name="mixer",
    )(
        me,
        step_bias,
        decay_log,
        skip_gain,
        *chunks,
        mix_gain.reshape(1, -1),
        w_step.T,
        conv_value,
        conv_maps,
        head_gain.reshape(1, -1),
        maps_near,
        *[
            in_hbm(a)
            for a in (
                past_value.transpose(1, 0, 2),
                past_maps.transpose(1, 0, 2),
                w_value,
                w_gate,
                state,
                w_out,
            )
        ],
    )

    parts = [part] + [shifted(part, size, step) for step in range(1, size)]
    up_near, down_near = fetch(part, [w_up, w_down], "fetch_mlp", 1e6)
    base, *pieces = pl.pallas_call(
        functools.partial(mlp_kernel, size),
        out_shape=[pltpu.VMEM((rows, width), f32)] + [pltpu.VMEM((rows, width), bf16)] * (size - 1),
        in_specs=[SMEM] + [VMEM] * (size + 4),
        out_specs=[VMEM] * size,
        scratch_shapes=[pltpu.VMEM((rows, model), f32), pltpu.VMEM((rows, model), f32)],
        compiler_params=pltpu.CompilerParams(vmem_limit_bytes=8 << 20),
        cost_estimate=cost(4 * rows * model * w_up.shape[1], 17e6),
        name="mlp",
    )(me, whole, *parts, mlp_gain.reshape(1, -1), up_near, down_near)

    arrived = [shifted(pieces[step - 1], size, step) for step in range(1, size)]
    held, decay, in_map, written, _ = lax.optimization_barrier((held, decay, in_map, written, base))
    state_next = pl.pallas_call(
        write_kernel,
        out_shape=jax.ShapeDtypeStruct(state.shape, f32),
        grid=(heads // 2,),
        in_specs=[VMEM] * 4,
        out_specs=pl.BlockSpec((rows, 2, HEAD_DIM, STATE), lambda pair: (0, pair, 0, 0)),
        compiler_params=pltpu.CompilerParams(vmem_limit_bytes=8 << 20),
        cost_estimate=cost(8e9, 25e6),
        name="write_state",
    )(held, decay, in_map, written)
    total = base
    for piece in arrived:
        total = total + piece.astype(f32)
    return (
        total.astype(bf16),
        state_next,
        value_tail.transpose(1, 0, 2),
        maps_tail.transpose(1, 0, 2),
    )


def local(size, *arrays):
    tokens, w_value, w_maps, state, w_up = (arrays[i] for i in (0, 3, 4, 14, 17))
    heads = state.shape[1]
    fits = (
        size <= 8
        and heads % 2 == 0
        and state.shape[2:] == (HEAD_DIM, STATE)
        and w_maps.shape[1] == heads * 2 * STATE
        and all(extent % TILE == 0 for extent in (w_value.shape[1], w_maps.shape[1], w_up.shape[1]))
        and tokens.shape[1] % LANES == 0
        and tokens.shape[0] % 8 == 0
    )
    return local_few(size, *arrays) if fits else local_many(*arrays)


def solution(mesh):
    in_specs = (
        P(("dp", "tp"), "kv"),
        P(),
        P(None, "kv"),
        P(None, "kv"),
        P(None, "kv"),
        P(),
        P(None, "kv"),
        P(None, "kv"),
        P(("dp", "tp"), None, "kv"),
        P(("dp", "tp"), None, "kv"),
        P("kv"),
        P("kv"),
        P("kv"),
        P("kv"),
        P(("dp", "tp"), "kv", None, None),
        P("kv", None),
        P(),
        P(None, "kv"),
        P("kv", None),
    )
    out_specs = (
        P(("dp", "tp"), "kv"),
        P(("dp", "tp"), "kv", None, None),
        P(("dp", "tp"), None, "kv"),
        P(("dp", "tp"), None, "kv"),
    )
    step = functools.partial(local, mesh.shape["kv"])
    return jax.shard_map(step, mesh=mesh, in_specs=in_specs, out_specs=out_specs, check_vma=False)
```

```python
import functools

import jax
import jax.numpy as jnp
from jax import lax
from jax.experimental import pallas as pl
from jax.experimental.pallas import tpu as pltpu
from jax.sharding import PartitionSpec as P

HEAD_DIM = 64
STATE = 128
LANES = 128
TILE = 1024
SLOTS = 3
GROUP = 4


NORM_EPS = 1e-05

VMEM = pl.BlockSpec(memory_space=pltpu.VMEM)
SMEM = pl.BlockSpec(memory_space=pltpu.SMEM)
HBM = pl.BlockSpec(memory_space=pltpu.HBM)


def rms_rows(matrix, gain_vec):
    widened = matrix.astype(jnp.float32)
    inv_scale = lax.rsqrt(jnp.mean(widened * widened, axis=-1, keepdims=True) + NORM_EPS)
    return (widened * inv_scale * gain_vec).astype(jnp.bfloat16)


def short_conv(past_rows, newest, kernel):
    window = jnp.concatenate([past_rows, newest[:, None, :]], axis=1)
    summed = jnp.sum(window.astype(jnp.float32) * kernel[None], axis=1)
    return (jax.nn.silu(summed), window[:, 1:, :])


def local_many(
    tokens,
    mix_gain,
    w_gate,
    w_value,
    w_maps,
    w_step,
    conv_value,
    conv_maps,
    past_value,
    past_maps,
    step_bias,
    decay_log,
    skip_gain,
    head_gain,
    state,
    w_out,
    mlp_gain,
    w_up,
    w_down,
):
    whole_rows = lax.all_gather(tokens, "kv", axis=1, tiled=True)
    batch_rows = whole_rows.shape[0]
    heads_here = state.shape[1]
    head_start = lax.axis_index("kv") * heads_here
    normed = rms_rows(whole_rows, mix_gain)
    gate_pre = jnp.dot(normed, w_gate, preferred_element_type=jnp.float32)
    step_cols = lax.dynamic_slice_in_dim(w_step, head_start, heads_here, 1)
    step_pre = jnp.dot(normed, step_cols, preferred_element_type=jnp.float32)
    value_new = jnp.dot(normed, w_value, preferred_element_type=jnp.float32).astype(jnp.bfloat16)
    maps_new = jnp.dot(normed, w_maps, preferred_element_type=jnp.float32).astype(jnp.bfloat16)
    value_act, value_tail = short_conv(past_value, value_new, conv_value)
    maps_act, maps_tail = short_conv(past_maps, maps_new, conv_maps)
    maps_act = lax.optimization_barrier(maps_act.astype(jnp.bfloat16))
    grouped = maps_act.astype(jnp.float32).reshape(batch_rows, -1, 2, STATE)
    per_group = heads_here // grouped.shape[1]
    in_map = jnp.repeat(grouped[:, :, 0], per_group, axis=1)
    out_map = jnp.repeat(grouped[:, :, 1], per_group, axis=1)
    head_values = value_act.reshape(batch_rows, heads_here, HEAD_DIM)
    step_size = jax.nn.softplus(step_pre + step_bias)
    decay_rate = jnp.exp(-step_size * jnp.exp(decay_log))
    written = (step_size[:, :, None] * head_values)[:, :, :, None] * in_map[:, :, None, :]
    state_next = decay_rate[:, :, None, None] * state + written
    read_out = (
        jnp.sum(state_next * out_map[:, :, None, :], axis=-1)
        + skip_gain[None, :, None] * head_values
    )
    gated_heads = read_out * jax.nn.silu(gate_pre.reshape(batch_rows, heads_here, HEAD_DIM))
    inv_scale = lax.rsqrt(jnp.mean(gated_heads * gated_heads, axis=-1, keepdims=True) + NORM_EPS)
    heads_out = gated_heads * inv_scale * head_gain.reshape(heads_here, HEAD_DIM)
    heads_out = heads_out.reshape(batch_rows, heads_here * HEAD_DIM).astype(jnp.bfloat16)
    partial_value = jnp.dot(heads_out, w_out, preferred_element_type=jnp.float32)
    own_part = lax.psum_scatter(partial_value, "kv", scatter_dimension=1, tiled=True)
    own_hidden = lax.optimization_barrier(
        (tokens.astype(jnp.float32) + own_part).astype(jnp.bfloat16)
    )
    hidden = lax.all_gather(own_hidden, "kv", axis=1, tiled=True)
    normed_mlp = rms_rows(hidden, mlp_gain)
    squared = jnp.square(jax.nn.relu(jnp.dot(normed_mlp, w_up, preferred_element_type=jnp.float32)))
    squared = squared.astype(jnp.bfloat16)
    partial_mlp = jnp.dot(squared, w_down, preferred_element_type=jnp.float32)
    mlp_part = lax.psum_scatter(partial_mlp, "kv", scatter_dimension=1, tiled=True)
    layer_out = (own_hidden.astype(jnp.float32) + mlp_part).astype(jnp.bfloat16)
    return (layer_out, state_next, value_tail, maps_tail)


def shifted(block, size, step):
    return lax.ppermute(block, "kv", [(i, (i + step) % size) for i in range(size)])


def in_hbm(array):
    return pltpu.with_memory_space_constraint(array, pltpu.HBM)


def cost(flops, moved):
    return pl.CostEstimate(flops=int(flops), bytes_accessed=int(moved), transcendentals=0)


def silu(x):
    return x / (1.0 + jnp.exp(-x))


def row_copies(source, target, sems, first, parts):
    depth = source.shape[0] // parts
    blocks = [pl.ds(part * depth, depth) for part in range(parts)]
    return [
        pltpu.make_async_copy(source.at[block], target.at[block], sems.at[first + part])
        for part, block in enumerate(blocks)
    ]


def fetch_kernel(parts, *refs):
    count = len(parts)
    sources, targets, sems = refs[:count], refs[count:-1], refs[-1]
    copies = []
    for source, target, number in zip(sources, targets, parts):
        copies += row_copies(source, target, sems, len(copies), number)
    for copy in copies:
        copy.start()
    for copy in copies:
        copy.wait()


def fetch(arrays, parts, name):
    moved = sum(a.size * a.dtype.itemsize for a in arrays)
    return pl.pallas_call(
        functools.partial(fetch_kernel, parts),
        out_shape=[pltpu.VMEM(a.shape, a.dtype) for a in arrays],
        in_specs=[HBM] * len(arrays),
        out_specs=[VMEM] * len(arrays),
        scratch_shapes=[pltpu.SemaphoreType.DMA((sum(parts),))],
        compiler_params=pltpu.CompilerParams(vmem_limit_bytes=1 << 20),
        cost_estimate=cost(1e6, 2 * moved),
        name=name,
    )(*[in_hbm(a) for a in arrays])


def mixer_kernel(size, *refs):
    me_ref, bias_ref, dlog_ref, skip_ref = refs[:4]
    chunks = refs[4 : 4 + size]
    (gain, wstep, conv_v, conv_m, hgain, wmaps, pastv_s, pastm_s, wvalue, wgate, state, wout) = refs[
        4 + size : 16 + size
    ]
    (part_o, x_o, state_o, dec_o, in_o, u_o, vtail, mtail) = refs[16 + size : 24 + size]
    (normed_s, wvalue_s, wgate_s, wout_s, newv_s, newm_s, out_s, value_s, gate_s, heads_s, sems, ssems) = refs[
        24 + size :
    ]
    rows, width = chunks[0].shape
    me = me_ref[0]
    heads = state.shape[1]
    pairs = heads // 2

    def state_copy(pair):
        both = pl.ds(2 * pair, 2)
        return pltpu.make_async_copy(state.at[:, both], state_o.at[:, both], ssems.at[pair])

    load_value = row_copies(wvalue, wvalue_s, sems, 0, 2)
    load_gate = row_copies(wgate, wgate_s, sems, 2, 2)
    load_out = row_copies(wout, wout_s, sems, 4, 2)
    later = pairs - 2
    tails = [
        pltpu.make_async_copy(pastm_s.at[pl.ds(1, 2)], mtail.at[pl.ds(0, 2)], sems.at[6]),
        pltpu.make_async_copy(pastv_s.at[pl.ds(1, 2)], vtail.at[pl.ds(0, 2)], sems.at[7]),
        pltpu.make_async_copy(newm_s, mtail.at[2], sems.at[8]),
        pltpu.make_async_copy(newv_s, vtail.at[2], sems.at[9]),
    ]

    for copy in load_value + load_gate:
        copy.start()

    for step in range(size):
        source = lax.rem(me + size - step, size)
        x_o[:, pl.ds(pl.multiple_of(source * width, width), width)] = chunks[step][...]
    x = x_o[...].astype(jnp.float32)
    inv = lax.rsqrt(jnp.mean(x * x, axis=-1, keepdims=True) + NORM_EPS)
    normed = (x * inv * gain[...]).astype(jnp.bfloat16)
    normed_s[...] = normed

    step_pre = lax.dot_general(
        normed, wstep[...], (((1,), (1,)), ((), ())), preferred_element_type=jnp.float32
    )

    def conv(past, new, taps, block):
        total = new.astype(jnp.float32) * taps[3:4, block]
        for t in range(3):
            total = total + past[t, :, block].astype(jnp.float32) * taps[t : t + 1, block]
        return silu(total)

    for copy in tails[:2]:
        copy.start()
    def span(index, extent):
        return pl.ds(pl.multiple_of(index * extent, extent), extent)

    def product(weights, block):
        return jnp.dot(normed_s[...], weights[:, block], preferred_element_type=jnp.float32)

    def maps_product(tile):
        block = span(tile, TILE)
        newm_s[:, block] = product(wmaps, block).astype(jnp.bfloat16)

    def maps_conv(tile):
        block = span(tile, TILE)
        act = conv(pastm_s, newm_s[:, block], conv_m, block).astype(jnp.bfloat16).astype(jnp.float32)
        groups = TILE // (2 * STATE)
        for group in range(groups):
            base = group * 2 * STATE
            target = span(tile * groups + group, STATE)
            in_o[:, target] = act[:, base : base + STATE]
            out_s[:, target] = act[:, base + STATE : base + 2 * STATE]

    def maps_body(tile, carry):
        for part in range(2):

            @pl.when(2 * tile + part < later)
            def _():
                state_copy(2 * tile + part).start()

        maps_product(tile + 1)
        maps_conv(tile)
        return carry

    last = wmaps.shape[1] // TILE - 1
    maps_product(0)
    lax.fori_loop(0, last, maps_body, 0)
    for pair in range(2 * last, later):
        state_copy(pair).start()
    for copy in load_value + load_gate:
        copy.wait()
    maps_conv(last)
    for tile in range(wvalue_s.shape[1] // TILE):
        block = pl.ds(tile * TILE, TILE)
        new = product(wvalue_s, block).astype(jnp.bfloat16)
        newv_s[:, block] = new
        value_s[:, block] = conv(pastv_s, new, conv_v, block)
        gate_s[:, block] = silu(product(wgate_s, block))
    for copy in tails[2:]:
        copy.start()

    row_of = lax.broadcasted_iota(jnp.int32, (rows, STATE), 0)
    part_of = lax.broadcasted_iota(jnp.int32, (rows, GROUP * HEAD_DIM), 1) // HEAD_DIM
    low = lax.broadcasted_iota(jnp.int32, (rows, LANES), 1) < HEAD_DIM
    step_lane = lax.broadcasted_iota(jnp.int32, step_pre.shape, 1)

    def carried_sums(group, outs):
        total = None
        for row in range(0, rows, 2):
            wanted = [
                jnp.concatenate([jnp.where(row_of == row + t, out, 0.0) for t in range(2)], axis=1)
                for out in outs
            ]
            held = [
                state_o[row + t, pl.ds(group * GROUP, GROUP)].reshape(GROUP * HEAD_DIM, STATE)
                for t in range(2)
            ]
            term = lax.dot_general(
                jnp.concatenate(wanted, axis=0).astype(jnp.bfloat16),
                jnp.concatenate(held, axis=1).astype(jnp.bfloat16),
                (((1,), (1,)), ((), ())),
                preferred_element_type=jnp.float32,
            )
            total = term if total is None else total + term
        picked = None
        for which in range(GROUP):
            piece = jnp.where(part_of == which, total[which * rows : (which + 1) * rows], 0.0)
            picked = piece if picked is None else picked + piece
        return picked

    def group_body(group, carry):
        for which in range(GROUP // 2):
            pair = group * (GROUP // 2) + which
            state_copy(pair).wait()

            @pl.when(pair + later < pairs)
            def _():
                state_copy(pair + later).start()

            for part in range(2):

                @pl.when(pair == pairs - later + part)
                def _():
                    load_out[part].start()

        outs, decays, sizes, meets = [], [], [], []
        for which in range(GROUP):
            head = group * GROUP + which
            wide = span(head, STATE)
            column = jnp.sum(
                jnp.where(step_lane == me * heads + head, step_pre, 0.0), axis=1, keepdims=True
            )
            pre = jnp.broadcast_to(column, (rows, LANES)) + bias_ref[head]
            size_h = jnp.maximum(pre, 0.0) + jnp.log1p(jnp.exp(-jnp.abs(pre)))
            rate = jnp.exp(jnp.full((rows, LANES), dlog_ref[head]))
            decay = jnp.exp(-size_h * rate)
            dec_o[:, wide] = decay
            outs.append(out_s[:, wide])
            meets.append(jnp.sum(in_o[:, wide] * outs[-1], axis=1, keepdims=True))
            decays.append(decay)
            sizes.append(size_h)
        carried = carried_sums(group, outs)
        for which in range(GROUP // 2):
            one, two = 2 * which, 2 * which + 1
            block = span(group * (GROUP // 2) + which, LANES)
            value = value_s[:, block]
            written = jnp.where(low, sizes[one], sizes[two]) * value
            u_o[:, block] = written
            read = jnp.where(low, decays[one], decays[two]) * carried[:, which * LANES : (which + 1) * LANES]
            read = read + jnp.where(low, meets[one], meets[two]) * written
            skip = jnp.where(low, skip_ref[group * GROUP + one], skip_ref[group * GROUP + two])
            gated = (read + skip * value) * gate_s[:, block]
            square = gated * gated
            first = jnp.sum(jnp.where(low, square, 0.0), axis=1, keepdims=True)
            second = jnp.sum(jnp.where(low, 0.0, square), axis=1, keepdims=True)
            scale = lax.rsqrt(jnp.where(low, first, second) * (1.0 / HEAD_DIM) + NORM_EPS)
            heads_s[:, block] = (gated * scale * hgain[:, block]).astype(jnp.bfloat16)
        return carry

    lax.fori_loop(0, heads // GROUP, group_body, 0)

    for copy in load_out:
        copy.wait()

    def out_body(tile, carry):
        block = span(tile, TILE)
        part_o[:, block] = jnp.dot(heads_s[...], wout_s[:, block], preferred_element_type=jnp.float32).astype(
            jnp.bfloat16
        )
        return carry

    lax.fori_loop(0, wout_s.shape[1] // TILE, out_body, 0)
    for copy in tails:
        copy.wait()


def write_kernel(parts, state_ref, dec_ref, in_ref, u_ref, wup, next_ref, wup_o, buffers, sems, wsems):
    rows, heads = state_ref.shape[:2]
    slots = buffers.shape[0]
    loads = row_copies(wup, wup_o, wsems, 0, parts)
    for copy in loads:
        copy.start()

    def store(pair):
        slot = lax.rem(pair, slots)
        return pltpu.make_async_copy(buffers.at[slot], next_ref.at[:, pl.ds(2 * pair, 2)], sems.at[slot])

    def pair_body(pair, carry):
        @pl.when(pair >= slots)
        def _():
            store(pair - slots).wait()

        slot = lax.rem(pair, slots)
        turned = jnp.transpose(u_ref[:, pl.ds(pl.multiple_of(pair * LANES, LANES), LANES)])
        for which in range(2):
            head = 2 * pair + which
            wide = pl.ds(pl.multiple_of(head * STATE, STATE), STATE)
            column = turned[which * HEAD_DIM : (which + 1) * HEAD_DIM]
            decay, in_map = dec_ref[:, wide], in_ref[:, wide]
            for row in range(rows):
                buffers[slot, row, which] = (
                    state_ref[row, head] * decay[row : row + 1]
                    + column[:, row : row + 1] * in_map[row : row + 1]
                )
        store(pair).start()
        return carry

    pairs = heads // 2
    lax.fori_loop(0, pairs, pair_body, 0)
    for pair in range(max(pairs - slots, 0), pairs):
        store(pair).wait()
    for copy in loads:
        copy.wait()


def mlp_kernel(size, *refs):
    me_ref, x_ref = refs[:2]
    parts = refs[2 : 2 + size]
    gain, wup, wdown = refs[2 + size : 5 + size]
    base_o = refs[5 + size]
    pieces = refs[6 + size : 5 + 2 * size]
    hidden_s, total_s, normed_s, squared_s, wdown_s, sems = refs[5 + 2 * size :]
    loads = row_copies(wdown, wdown_s, sems, 0, sems.shape[0])
    for copy in loads:
        copy.start()
    width = base_o.shape[1]
    me = me_ref[0]
    total = x_ref[...].astype(jnp.float32)
    for part in parts:
        total = total + part[...].astype(jnp.float32)
    hidden = total.astype(jnp.bfloat16)
    hidden_s[...] = hidden.astype(jnp.float32)
    wide = hidden_s[...]
    inv = lax.rsqrt(jnp.mean(wide * wide, axis=-1, keepdims=True) + NORM_EPS)
    normed = (wide * inv * gain[...]).astype(jnp.bfloat16)
    normed_s[...] = normed

    def up_body(tile, carry):
        block = pl.ds(pl.multiple_of(tile * TILE, TILE), TILE)
        up = jnp.maximum(jnp.dot(normed_s[...], wup[:, block], preferred_element_type=jnp.float32), 0.0)
        squared_s[:, block] = (up * up).astype(jnp.bfloat16)
        return carry

    lax.fori_loop(0, wup.shape[1] // TILE, up_body, 0)
    out = None
    depth = wdown.shape[0] // len(loads)
    for part, copy in enumerate(loads):
        copy.wait()
        block = pl.ds(part * depth, depth)
        down = jnp.dot(squared_s[:, block], wdown_s[block, :], preferred_element_type=jnp.float32)
        out = down if out is None else out + down
    total_s[...] = out
    own = pl.ds(pl.multiple_of(me * width, width), width)
    base_o[...] = hidden_s[:, own] + total_s[:, own]
    for step in range(1, size):
        target = lax.rem(me + step, size)
        block = pl.ds(pl.multiple_of(target * width, width), width)
        pieces[step - 1][...] = total_s[:, block].astype(jnp.bfloat16)


def local_few(
    size,
    tokens,
    mix_gain,
    w_gate,
    w_value,
    w_maps,
    w_step,
    conv_value,
    conv_maps,
    past_value,
    past_maps,
    step_bias,
    decay_log,
    skip_gain,
    head_gain,
    state,
    w_out,
    mlp_gain,
    w_up,
    w_down,
):
    f32, bf16 = jnp.float32, jnp.bfloat16
    rows, width = tokens.shape
    model = width * size
    heads = state.shape[1]
    inner, maps = w_value.shape[1], w_maps.shape[1]
    me = lax.axis_index("kv").astype(jnp.int32).reshape(1)

    chunks = [tokens] + [shifted(tokens, size, step) for step in range(1, size)]
    past_value, past_maps = past_value.transpose(1, 0, 2), past_maps.transpose(1, 0, 2)
    maps_near, value_near, past_near = fetch([w_maps, past_value, past_maps], (8, 1, 1), "fetch_maps")
    part, whole, held, decay, in_map, written, value_tail, maps_tail = pl.pallas_call(
        functools.partial(mixer_kernel, size),
        out_shape=[
            pltpu.VMEM((rows, model), bf16),
            pltpu.VMEM((rows, model), bf16),
            pltpu.VMEM(state.shape, f32),
            pltpu.VMEM((rows, heads * STATE), f32),
            pltpu.VMEM((rows, heads * STATE), f32),
            pltpu.VMEM((rows, inner), f32),
            jax.ShapeDtypeStruct((3, rows, inner), bf16),
            jax.ShapeDtypeStruct((3, rows, maps), bf16),
        ],
        in_specs=[SMEM] * 4 + [VMEM] * (size + 8) + [HBM] * 4,
        out_specs=[VMEM] * 6 + [HBM] * 2,
        scratch_shapes=[
            pltpu.VMEM((rows, model), bf16),
            pltpu.VMEM(w_value.shape, bf16),
            pltpu.VMEM(w_gate.shape, bf16),
            pltpu.VMEM(w_out.shape, bf16),
            pltpu.VMEM((rows, inner), bf16),
            pltpu.VMEM((rows, maps), bf16),
            pltpu.VMEM((rows, heads * STATE), f32),
            pltpu.VMEM((rows, inner), f32),
            pltpu.VMEM((rows, inner), f32),
            pltpu.VMEM((rows, inner), bf16),
            pltpu.SemaphoreType.DMA((10,)),
            pltpu.SemaphoreType.DMA((heads // 2,)),
        ],
        compiler_params=pltpu.CompilerParams(vmem_limit_bytes=20 << 20),
        cost_estimate=cost(2 * rows * model * (2 * inner + maps), 40e6),
        name="mixer",
    )(
        me,
        step_bias,
        decay_log,
        skip_gain,
        *chunks,
        mix_gain.reshape(1, -1),
        w_step.T,
        conv_value,
        conv_maps,
        head_gain.reshape(1, -1),
        maps_near,
        value_near,
        past_near,
        *[in_hbm(a) for a in (w_value, w_gate, state, w_out)],
    )

    parts = [part] + [shifted(part, size, step) for step in range(1, size)]
    state_next, up_near = pl.pallas_call(
        functools.partial(write_kernel, 4),
        out_shape=[jax.ShapeDtypeStruct(state.shape, f32), pltpu.VMEM(w_up.shape, bf16)],
        in_specs=[VMEM] * 4 + [HBM],
        out_specs=[HBM, VMEM],
        scratch_shapes=[
            pltpu.VMEM((SLOTS, rows, 2, HEAD_DIM, STATE), f32),
            pltpu.SemaphoreType.DMA((SLOTS,)),
            pltpu.SemaphoreType.DMA((4,)),
        ],
        compiler_params=pltpu.CompilerParams(vmem_limit_bytes=8 << 20),
        cost_estimate=cost(1e6, 33e6),
        name="write_state",
    )(held, decay, in_map, written, in_hbm(w_up))
    base, *pieces = pl.pallas_call(
        functools.partial(mlp_kernel, size),
        out_shape=[pltpu.VMEM((rows, width), f32)] + [pltpu.VMEM((rows, width), bf16)] * (size - 1),
        in_specs=[SMEM] + [VMEM] * (size + 3) + [HBM],
        out_specs=[VMEM] * size,
        scratch_shapes=[
            pltpu.VMEM((rows, model), f32),
            pltpu.VMEM((rows, model), f32),
            pltpu.VMEM((rows, model), bf16),
            pltpu.VMEM((rows, w_up.shape[1]), bf16),
            pltpu.VMEM(w_down.shape, bf16),
            pltpu.SemaphoreType.DMA((4,)),
        ],
        compiler_params=pltpu.CompilerParams(vmem_limit_bytes=12 << 20),
        cost_estimate=cost(4 * rows * model * w_up.shape[1], 17e6),
        name="mlp",
    )(me, whole, *parts, mlp_gain.reshape(1, -1), up_near, in_hbm(w_down))

    arrived = [shifted(pieces[step - 1], size, step) for step in range(1, size)]
    total = base
    for piece in arrived:
        total = total + piece.astype(f32)
    return (
        total.astype(bf16),
        state_next,
        value_tail.transpose(1, 0, 2),
        maps_tail.transpose(1, 0, 2),
    )


def local(size, *arrays):
    tokens, w_value, w_maps, state, w_up = (arrays[i] for i in (0, 3, 4, 14, 17))
    heads = state.shape[1]
    fits = (
        size <= 8
        and heads % GROUP == 0
        and state.shape[2:] == (HEAD_DIM, STATE)
        and w_maps.shape[1] == heads * 2 * STATE
        and all(extent % TILE == 0 for extent in (w_value.shape[1], w_maps.shape[1], w_up.shape[1]))
        and tokens.shape[1] % LANES == 0
        and tokens.shape[0] % 8 == 0
    )
    return local_few(size, *arrays) if fits else local_many(*arrays)


def solution(mesh):
    in_specs = (
        P(("dp", "tp"), "kv"),
        P(),
        P(None, "kv"),
        P(None, "kv"),
        P(None, "kv"),
        P(),
        P(None, "kv"),
        P(None, "kv"),
        P(("dp", "tp"), None, "kv"),
        P(("dp", "tp"), None, "kv"),
        P("kv"),
        P("kv"),
        P("kv"),
        P("kv"),
        P(("dp", "tp"), "kv", None, None),
        P("kv", None),
        P(),
        P(None, "kv"),
        P("kv", None),
    )
    out_specs = (
        P(("dp", "tp"), "kv"),
        P(("dp", "tp"), "kv", None, None),
        P(("dp", "tp"), None, "kv"),
        P(("dp", "tp"), None, "kv"),
    )
    step = functools.partial(local, mesh.shape["kv"])
    return jax.shard_map(step, mesh=mesh, in_specs=in_specs, out_specs=out_specs, check_vma=False)
```

```python
import functools

import jax
import jax.numpy as jnp
from jax import lax
from jax.experimental import pallas as pl
from jax.experimental.pallas import tpu as pltpu
from jax.sharding import PartitionSpec as P

HEAD_DIM = 64
STATE = 128
LANES = 128
TILE = 1024
SLOTS = 3
LATE = 3
GROUP = 4


NORM_EPS = 1e-05

VMEM = pl.BlockSpec(memory_space=pltpu.VMEM)
HBM = pl.BlockSpec(memory_space=pltpu.HBM)


def rms_rows(matrix, gain_vec):
    widened = matrix.astype(jnp.float32)
    inv_scale = lax.rsqrt(jnp.mean(widened * widened, axis=-1, keepdims=True) + NORM_EPS)
    return (widened * inv_scale * gain_vec).astype(jnp.bfloat16)


def short_conv(past_rows, newest, kernel):
    window = jnp.concatenate([past_rows, newest[:, None, :]], axis=1)
    summed = jnp.sum(window.astype(jnp.float32) * kernel[None], axis=1)
    return (jax.nn.silu(summed), window[:, 1:, :])


def local_many(
    tokens,
    mix_gain,
    w_gate,
    w_value,
    w_maps,
    w_step,
    conv_value,
    conv_maps,
    past_value,
    past_maps,
    step_bias,
    decay_log,
    skip_gain,
    head_gain,
    state,
    w_out,
    mlp_gain,
    w_up,
    w_down,
):
    whole_rows = lax.all_gather(tokens, "kv", axis=1, tiled=True)
    batch_rows = whole_rows.shape[0]
    heads_here = state.shape[1]
    head_start = lax.axis_index("kv") * heads_here
    normed = rms_rows(whole_rows, mix_gain)
    gate_pre = jnp.dot(normed, w_gate, preferred_element_type=jnp.float32)
    step_cols = lax.dynamic_slice_in_dim(w_step, head_start, heads_here, 1)
    step_pre = jnp.dot(normed, step_cols, preferred_element_type=jnp.float32)
    value_new = jnp.dot(normed, w_value, preferred_element_type=jnp.float32).astype(jnp.bfloat16)
    maps_new = jnp.dot(normed, w_maps, preferred_element_type=jnp.float32).astype(jnp.bfloat16)
    value_act, value_tail = short_conv(past_value, value_new, conv_value)
    maps_act, maps_tail = short_conv(past_maps, maps_new, conv_maps)
    maps_act = lax.optimization_barrier(maps_act.astype(jnp.bfloat16))
    grouped = maps_act.astype(jnp.float32).reshape(batch_rows, -1, 2, STATE)
    per_group = heads_here // grouped.shape[1]
    in_map = jnp.repeat(grouped[:, :, 0], per_group, axis=1)
    out_map = jnp.repeat(grouped[:, :, 1], per_group, axis=1)
    head_values = value_act.reshape(batch_rows, heads_here, HEAD_DIM)
    step_size = jax.nn.softplus(step_pre + step_bias)
    decay_rate = jnp.exp(-step_size * jnp.exp(decay_log))
    written = (step_size[:, :, None] * head_values)[:, :, :, None] * in_map[:, :, None, :]
    state_next = decay_rate[:, :, None, None] * state + written
    read_out = (
        jnp.sum(state_next * out_map[:, :, None, :], axis=-1)
        + skip_gain[None, :, None] * head_values
    )
    gated_heads = read_out * jax.nn.silu(gate_pre.reshape(batch_rows, heads_here, HEAD_DIM))
    inv_scale = lax.rsqrt(jnp.mean(gated_heads * gated_heads, axis=-1, keepdims=True) + NORM_EPS)
    heads_out = gated_heads * inv_scale * head_gain.reshape(heads_here, HEAD_DIM)
    heads_out = heads_out.reshape(batch_rows, heads_here * HEAD_DIM).astype(jnp.bfloat16)
    partial_value = jnp.dot(heads_out, w_out, preferred_element_type=jnp.float32)
    own_part = lax.psum_scatter(partial_value, "kv", scatter_dimension=1, tiled=True)
    own_hidden = lax.optimization_barrier(
        (tokens.astype(jnp.float32) + own_part).astype(jnp.bfloat16)
    )
    hidden = lax.all_gather(own_hidden, "kv", axis=1, tiled=True)
    normed_mlp = rms_rows(hidden, mlp_gain)
    squared = jnp.square(jax.nn.relu(jnp.dot(normed_mlp, w_up, preferred_element_type=jnp.float32)))
    squared = squared.astype(jnp.bfloat16)
    partial_mlp = jnp.dot(squared, w_down, preferred_element_type=jnp.float32)
    mlp_part = lax.psum_scatter(partial_mlp, "kv", scatter_dimension=1, tiled=True)
    layer_out = (own_hidden.astype(jnp.float32) + mlp_part).astype(jnp.bfloat16)
    return (layer_out, state_next, value_tail, maps_tail)


def swapped(block, size, step):
    return lax.ppermute(block, "kv", [(i, i ^ step) for i in range(size)])


def shifted(block, size, step):
    return lax.ppermute(block, "kv", [(i, (i + step) % size) for i in range(size)])


def in_hbm(array):
    return pltpu.with_memory_space_constraint(array, pltpu.HBM)


def cost(flops, moved):
    return pl.CostEstimate(flops=int(flops), bytes_accessed=int(moved), transcendentals=0)


def silu(x):
    return x / (1.0 + jnp.exp(-x))


def row_copies(source, target, sems, first, parts):
    depth = source.shape[0] // parts
    blocks = [pl.ds(part * depth, depth) for part in range(parts)]
    return [
        pltpu.make_async_copy(source.at[block], target.at[block], sems.at[first + part])
        for part, block in enumerate(blocks)
    ]


def fetch_kernel(parts, *refs):
    count = len(parts)
    sources, targets, sems = refs[:count], refs[count:-1], refs[-1]
    copies = []
    for source, target, number in zip(sources, targets, parts):
        copies += row_copies(source, target, sems, len(copies), number)
    for copy in copies:
        copy.start()
    for copy in copies:
        copy.wait()


def fetch(arrays, parts, name):
    moved = sum(a.size * a.dtype.itemsize for a in arrays)
    return pl.pallas_call(
        functools.partial(fetch_kernel, parts),
        out_shape=[pltpu.VMEM(a.shape, a.dtype) for a in arrays],
        in_specs=[HBM] * len(arrays),
        out_specs=[VMEM] * len(arrays),
        scratch_shapes=[pltpu.SemaphoreType.DMA((sum(parts),))],
        compiler_params=pltpu.CompilerParams(vmem_limit_bytes=1 << 20),
        cost_estimate=cost(1e6, 2 * moved),
        name=name,
    )(*[in_hbm(a) for a in arrays])


def mixer_kernel(size, *refs):
    bias_ref, dlog_ref, skip_ref = refs[:3]
    refs = refs[3:]
    chunks = refs[:size]
    (gain, wstep, conv_v, conv_m, hgain, wmaps, pastv_s, pastm_s, wvalue, wgate, state, wout) = refs[
        size : 12 + size
    ]
    (part_o, x_o, state_o, dec_o, in_o, u_o, vtail, mtail) = refs[12 + size : 20 + size]
    (normed_s, wboth_s, raw_s, wout_s, newv_s, newm_s, out_s, value_s, gate_s, heads_s, sems, ssems) = refs[
        20 + size :
    ]
    rows, width = chunks[0].shape
    me = lax.axis_index("kv")
    heads = state.shape[1]
    pairs = heads // 2

    def state_copy(pair):
        both = pl.ds(2 * pair, 2)
        return pltpu.make_async_copy(state.at[:, both], state_o.at[:, both], ssems.at[pair])

    inner = wvalue.shape[1]
    load_value = row_copies(wvalue, wboth_s.at[:, pl.ds(0, inner)], sems, 0, 2)
    load_gate = row_copies(wgate, wboth_s.at[:, pl.ds(inner, inner)], sems, 2, 2)
    load_out = row_copies(wout, wout_s, sems, 4, 2)
    later = pairs - 2
    tails = [
        pltpu.make_async_copy(pastm_s.at[pl.ds(1, 2)], mtail.at[pl.ds(0, 2)], sems.at[6]),
        pltpu.make_async_copy(pastv_s.at[pl.ds(1, 2)], vtail.at[pl.ds(0, 2)], sems.at[7]),
        pltpu.make_async_copy(newm_s, mtail.at[2], sems.at[8]),
        pltpu.make_async_copy(newv_s, vtail.at[2], sems.at[9]),
    ]

    for copy in load_value + load_gate:
        copy.start()

    for step in range(size):
        source = lax.bitwise_xor(me, step)
        x_o[:, pl.ds(pl.multiple_of(source * width, width), width)] = chunks[step][...]
    x = x_o[...].astype(jnp.float32)
    inv = lax.rsqrt(jnp.mean(x * x, axis=-1, keepdims=True) + NORM_EPS)
    normed = (x * inv * gain[...]).astype(jnp.bfloat16)
    normed_s[...] = normed

    step_pre = lax.dot_general(
        normed, wstep[...], (((1,), (1,)), ((), ())), preferred_element_type=jnp.float32
    )

    def conv(past, new, taps, block):
        total = new.astype(jnp.float32) * taps[3:4, block]
        for t in range(3):
            total = total + past[t, :, block].astype(jnp.float32) * taps[t : t + 1, block]
        return silu(total)

    for copy in tails[:2]:
        copy.start()
    def span(index, extent):
        return pl.ds(pl.multiple_of(index * extent, extent), extent)

    def product(weights, block):
        return jnp.dot(normed_s[...], weights[:, block], preferred_element_type=jnp.float32)

    def maps_conv(tile):
        block = span(tile, TILE)
        act = conv(pastm_s, newm_s[:, block], conv_m, block).astype(jnp.bfloat16).astype(jnp.float32)
        groups = TILE // (2 * STATE)
        for group in range(groups):
            base = group * 2 * STATE
            target = span(tile * groups + group, STATE)
            in_o[:, target] = act[:, base : base + STATE]
            out_s[:, target] = act[:, base + STATE : base + 2 * STATE]

    def maps_body(tile, carry):
        @pl.when(tile < later)
        def _():
            state_copy(tile).start()

        maps_conv(jnp.maximum(tile - 1, 0))
        block = span(tile, TILE)
        newm_s[:, block] = product(wmaps, block).astype(jnp.bfloat16)
        return carry

    tiles = wmaps.shape[1] // TILE
    newm_s[:, :TILE] = jnp.zeros((rows, TILE), jnp.bfloat16)
    lax.fori_loop(0, tiles, maps_body, 0)
    for pair in range(tiles, later):
        state_copy(pair).start()
    tails[2].start()
    for copy in load_value + load_gate:
        copy.wait()

    def raw_body(tile, carry):
        block = span(tile, TILE)
        raw_s[:, block] = product(wboth_s, block)
        return carry

    maps_conv(tiles - 1)
    lax.fori_loop(0, 2 * inner // TILE, raw_body, 0)

    def value_body(tile, carry):
        block = span(tile, TILE)
        new = raw_s[:, block].astype(jnp.bfloat16)
        newv_s[:, block] = new
        value_s[:, block] = conv(pastv_s, new, conv_v, block)
        gate_s[:, block] = silu(raw_s[:, span(tile + inner // TILE, TILE)])
        return carry

    lax.fori_loop(0, inner // TILE, value_body, 0)
    tails[3].start()

    row_of = lax.broadcasted_iota(jnp.int32, (rows, STATE), 0)
    part_of = lax.broadcasted_iota(jnp.int32, (rows, GROUP * HEAD_DIM), 1) // HEAD_DIM
    low = lax.broadcasted_iota(jnp.int32, (rows, LANES), 1) < HEAD_DIM
    step_lane = lax.broadcasted_iota(jnp.int32, step_pre.shape, 1)
    head_lane = lax.broadcasted_iota(jnp.int32, (1, heads), 1)

    def of_head(ref, head):
        return jnp.sum(jnp.where(head_lane == head, ref[...], 0.0), axis=1, keepdims=True)

    def carried_sums(group, outs):
        total = None
        for row in range(0, rows, 2):
            wanted = [
                jnp.concatenate([jnp.where(row_of == row + t, out, 0.0) for t in range(2)], axis=1)
                for out in outs
            ]
            held = [
                state_o[row + t, pl.ds(group * GROUP, GROUP)].reshape(GROUP * HEAD_DIM, STATE)
                for t in range(2)
            ]
            term = lax.dot_general(
                jnp.concatenate(wanted, axis=0).astype(jnp.bfloat16),
                jnp.concatenate(held, axis=1).astype(jnp.bfloat16),
                (((1,), (1,)), ((), ())),
                preferred_element_type=jnp.float32,
            )
            total = term if total is None else total + term
        picked = None
        for which in range(GROUP):
            piece = jnp.where(part_of == which, total[which * rows : (which + 1) * rows], 0.0)
            picked = piece if picked is None else picked + piece
        return picked

    def group_body(group, carry):
        for which in range(GROUP // 2):
            pair = group * (GROUP // 2) + which
            state_copy(pair).wait()

            @pl.when(pair + later < pairs)
            def _():
                state_copy(pair + later).start()

            for part in range(2):

                @pl.when(pair == pairs - later + part)
                def _():
                    load_out[part].start()

        outs, decays, sizes, meets = [], [], [], []
        for which in range(GROUP):
            head = group * GROUP + which
            wide = span(head, STATE)
            column = jnp.sum(
                jnp.where(step_lane == me * heads + head, step_pre, 0.0), axis=1, keepdims=True
            )
            pre = jnp.broadcast_to(column, (rows, LANES)) + of_head(bias_ref, head)
            size_h = jnp.maximum(pre, 0.0) + jnp.log1p(jnp.exp(-jnp.abs(pre)))
            rate = jnp.exp(of_head(dlog_ref, head))
            decay = jnp.exp(-size_h * rate)
            dec_o[:, wide] = decay
            outs.append(out_s[:, wide])
            meets.append(jnp.sum(in_o[:, wide] * outs[-1], axis=1, keepdims=True))
            decays.append(decay)
            sizes.append(size_h)
        carried = carried_sums(group, outs)
        for which in range(GROUP // 2):
            one, two = 2 * which, 2 * which + 1
            block = span(group * (GROUP // 2) + which, LANES)
            value = value_s[:, block]
            written = jnp.where(low, sizes[one], sizes[two]) * value
            u_o[:, block] = written
            read = jnp.where(low, decays[one], decays[two]) * carried[:, which * LANES : (which + 1) * LANES]
            read = read + jnp.where(low, meets[one], meets[two]) * written
            skip = jnp.where(low, of_head(skip_ref, group * GROUP + one), of_head(skip_ref, group * GROUP + two))
            gated = (read + skip * value) * gate_s[:, block]
            square = gated * gated
            first = jnp.sum(jnp.where(low, square, 0.0), axis=1, keepdims=True)
            second = jnp.sum(jnp.where(low, 0.0, square), axis=1, keepdims=True)
            scale = lax.rsqrt(jnp.where(low, first, second) * (1.0 / HEAD_DIM) + NORM_EPS)
            heads_s[:, block] = (gated * scale * hgain[:, block]).astype(jnp.bfloat16)
        return carry

    lax.fori_loop(0, heads // GROUP, group_body, 0)

    half = inner // 2
    load_out[0].wait()

    def first_body(tile, carry):
        block = span(tile, TILE)
        raw_s[:, block] = jnp.dot(heads_s[:, :half], wout_s[:half, block], preferred_element_type=jnp.float32)
        return carry

    def second_body(tile, carry):
        block = span(tile, TILE)
        rest = jnp.dot(heads_s[:, half:], wout_s[half:, block], preferred_element_type=jnp.float32)
        part_o[:, block] = (raw_s[:, block] + rest).astype(jnp.bfloat16)
        return carry

    lax.fori_loop(0, wout_s.shape[1] // TILE, first_body, 0)
    load_out[1].wait()
    lax.fori_loop(0, wout_s.shape[1] // TILE, second_body, 0)
    for copy in tails:
        copy.wait()


def write_pairs(first, last, state_ref, dec_ref, in_ref, u_ref, next_ref, buffers, sems):
    rows = state_ref.shape[0]
    slots = buffers.shape[0]

    def store(pair, which):
        slot = lax.rem(pair, slots)
        return pltpu.make_async_copy(
            buffers.at[slot, which], next_ref.at[:, 2 * pair + which], sems.at[slot, which]
        )

    def pair_body(pair, carry):
        slot = lax.rem(pair, slots)
        turned = jnp.transpose(u_ref[:, pl.ds(pl.multiple_of(pair * LANES, LANES), LANES)])
        for which in range(2):

            @pl.when(pair >= first + slots)
            def _():
                store(pair - slots, which).wait()

            head = 2 * pair + which
            wide = pl.ds(pl.multiple_of(head * STATE, STATE), STATE)
            column = turned[which * HEAD_DIM : (which + 1) * HEAD_DIM]
            decay, in_map = dec_ref[:, wide], in_ref[:, wide]
            for row in range(rows):
                buffers[slot, which, row] = (
                    state_ref[row, head] * decay[row : row + 1]
                    + column[:, row : row + 1] * in_map[row : row + 1]
                )
            store(pair, which).start()
        return carry

    lax.fori_loop(first, last, pair_body, 0)
    for pair in range(max(last - slots, first), last):
        for which in range(2):
            store(pair, which).wait()


def early_kernel(first, last, parts, *refs):
    wup, next_ref, wup_o, buffers, sems, wsems = refs[4:]
    loads = row_copies(wup, wup_o, wsems, 0, parts)
    for copy in loads:
        copy.start()
    write_pairs(first, last, *refs[:4], next_ref, buffers, sems)
    for copy in loads:
        copy.wait()


def late_kernel(first, last, *refs):
    next_ref, buffers, sems = refs[5:]
    write_pairs(first, last, *refs[:4], next_ref, buffers, sems)


def mlp_kernel(size, *refs):
    x_ref = refs[0]
    parts = refs[1 : 1 + size]
    gain, wup, wdown = refs[1 + size : 4 + size]
    base_o = refs[4 + size]
    pieces = refs[5 + size : 4 + 2 * size]
    hidden_s, total_s, normed_s, squared_s, wdown_s, sems = refs[4 + 2 * size :]
    loads = row_copies(wdown, wdown_s, sems, 0, sems.shape[0])
    for copy in loads:
        copy.start()
    width = base_o.shape[1]
    me = lax.axis_index("kv")
    total = x_ref[...].astype(jnp.float32)
    for part in parts:
        total = total + part[...].astype(jnp.float32)
    hidden = total.astype(jnp.bfloat16)
    hidden_s[...] = hidden.astype(jnp.float32)
    wide = hidden_s[...]
    inv = lax.rsqrt(jnp.mean(wide * wide, axis=-1, keepdims=True) + NORM_EPS)
    normed = (wide * inv * gain[...]).astype(jnp.bfloat16)
    normed_s[...] = normed

    def up_body(tile, carry):
        block = pl.ds(pl.multiple_of(tile * TILE, TILE), TILE)
        up = jnp.maximum(jnp.dot(normed_s[...], wup[:, block], preferred_element_type=jnp.float32), 0.0)
        squared_s[:, block] = (up * up).astype(jnp.bfloat16)
        return carry

    lax.fori_loop(0, wup.shape[1] // TILE, up_body, 0)
    depth = wdown.shape[0] // sems.shape[0]
    total_s[...] = jnp.zeros(total_s.shape, jnp.float32)

    def down_body(part, carry):
        block = pl.ds(pl.multiple_of(part * depth, depth), depth)
        pltpu.make_async_copy(wdown.at[block], wdown_s.at[block], sems.at[part]).wait()
        total_s[...] += jnp.dot(squared_s[:, block], wdown_s[block, :], preferred_element_type=jnp.float32)
        return carry

    lax.fori_loop(0, sems.shape[0], down_body, 0)
    own = pl.ds(pl.multiple_of(me * width, width), width)
    base_o[...] = hidden_s[:, own] + total_s[:, own]
    for step in range(1, size):
        target = lax.rem(me + step, size)
        block = pl.ds(pl.multiple_of(target * width, width), width)
        pieces[step - 1][...] = total_s[:, block].astype(jnp.bfloat16)


def local_few(
    size,
    tokens,
    mix_gain,
    w_gate,
    w_value,
    w_maps,
    w_step,
    conv_value,
    conv_maps,
    past_value,
    past_maps,
    step_bias,
    decay_log,
    skip_gain,
    head_gain,
    state,
    w_out,
    mlp_gain,
    w_up,
    w_down,
):
    f32, bf16 = jnp.float32, jnp.bfloat16
    rows, width = tokens.shape
    model = width * size
    heads = state.shape[1]
    inner, maps = w_value.shape[1], w_maps.shape[1]

    chunks = [tokens] + [swapped(tokens, size, step) for step in range(1, size)]
    past_value, past_maps = past_value.transpose(1, 0, 2), past_maps.transpose(1, 0, 2)
    maps_near, value_near, past_near = fetch([w_maps, past_value, past_maps], (8, 1, 1), "fetch_maps")
    part, whole, held, decay, in_map, written, value_tail, maps_tail = pl.pallas_call(
        functools.partial(mixer_kernel, size),
        out_shape=[
            pltpu.VMEM((rows, model), bf16),
            pltpu.VMEM((rows, model), bf16),
            pltpu.VMEM(state.shape, f32),
            pltpu.VMEM((rows, heads * STATE), f32),
            pltpu.VMEM((rows, heads * STATE), f32),
            pltpu.VMEM((rows, inner), f32),
            jax.ShapeDtypeStruct((3, rows, inner), bf16),
            jax.ShapeDtypeStruct((3, rows, maps), bf16),
        ],
        in_specs=[VMEM] * (size + 11) + [HBM] * 4,
        out_specs=[VMEM] * 6 + [HBM] * 2,
        scratch_shapes=[
            pltpu.VMEM((rows, model), bf16),
            pltpu.VMEM((model, 2 * inner), bf16),
            pltpu.VMEM((rows, max(2 * inner, model)), f32),
            pltpu.VMEM(w_out.shape, bf16),
            pltpu.VMEM((rows, inner), bf16),
            pltpu.VMEM((rows, maps), bf16),
            pltpu.VMEM((rows, heads * STATE), f32),
            pltpu.VMEM((rows, inner), f32),
            pltpu.VMEM((rows, inner), f32),
            pltpu.VMEM((rows, inner), bf16),
            pltpu.SemaphoreType.DMA((10,)),
            pltpu.SemaphoreType.DMA((heads // 2,)),
        ],
        compiler_params=pltpu.CompilerParams(vmem_limit_bytes=20 << 20),
        cost_estimate=cost(2 * rows * model * (2 * inner + maps), 40e6),
        name="mixer",
    )(
        step_bias.reshape(1, -1),
        decay_log.reshape(1, -1),
        skip_gain.reshape(1, -1),
        *chunks,
        mix_gain.reshape(1, -1),
        w_step.T,
        conv_value,
        conv_maps,
        head_gain.reshape(1, -1),
        maps_near,
        value_near,
        past_near,
        *[in_hbm(a) for a in (w_value, w_gate, state, w_out)],
    )

    parts = [part] + [shifted(part, size, step) for step in range(1, size)]
    pairs = heads // 2
    middle = pairs - pairs * LATE // 8
    state_first, up_near = pl.pallas_call(
        functools.partial(early_kernel, 0, middle, 4),
        out_shape=[jax.ShapeDtypeStruct(state.shape, f32), pltpu.VMEM(w_up.shape, bf16)],
        in_specs=[VMEM] * 4 + [HBM],
        out_specs=[HBM, VMEM],
        scratch_shapes=[
            pltpu.VMEM((SLOTS, 2, rows, HEAD_DIM, STATE), f32),
            pltpu.SemaphoreType.DMA((SLOTS, 2)),
            pltpu.SemaphoreType.DMA((4,)),
        ],
        compiler_params=pltpu.CompilerParams(vmem_limit_bytes=8 << 20),
        cost_estimate=cost(1e6, 33e6),
        name="write_early",
    )(held, decay, in_map, written, in_hbm(w_up))
    base, *pieces = pl.pallas_call(
        functools.partial(mlp_kernel, size),
        out_shape=[pltpu.VMEM((rows, width), f32)] + [pltpu.VMEM((rows, width), bf16)] * (size - 1),
        in_specs=[VMEM] * (size + 3) + [HBM],
        out_specs=[VMEM] * size,
        scratch_shapes=[
            pltpu.VMEM((rows, model), f32),
            pltpu.VMEM((rows, model), f32),
            pltpu.VMEM((rows, model), bf16),
            pltpu.VMEM((rows, w_up.shape[1]), bf16),
            pltpu.VMEM(w_down.shape, bf16),
            pltpu.SemaphoreType.DMA((4,)),
        ],
        compiler_params=pltpu.CompilerParams(vmem_limit_bytes=12 << 20),
        cost_estimate=cost(4 * rows * model * w_up.shape[1], 17e6),
        name="mlp",
    )(whole, *parts, mlp_gain.reshape(1, -1), up_near, in_hbm(w_down))

    arrived = [shifted(pieces[step - 1], size, step) for step in range(size - 1, 0, -1)]
    held, decay, in_map, written, _ = lax.optimization_barrier((held, decay, in_map, written, base))
    state_next = pl.pallas_call(
        functools.partial(late_kernel, middle, pairs),
        out_shape=jax.ShapeDtypeStruct(state.shape, f32),
        in_specs=[VMEM] * 4 + [HBM],
        out_specs=HBM,
        scratch_shapes=[
            pltpu.VMEM((SLOTS, 2, rows, HEAD_DIM, STATE), f32),
            pltpu.SemaphoreType.DMA((SLOTS, 2)),
        ],
        input_output_aliases={4: 0},
        compiler_params=pltpu.CompilerParams(vmem_limit_bytes=8 << 20),
        cost_estimate=cost(1e6, 1e7),
        name="write_late",
    )(held, decay, in_map, written, in_hbm(state_first))
    total = base
    for piece in arrived:
        total = total + piece.astype(f32)
    return (
        total.astype(bf16),
        state_next,
        value_tail.transpose(1, 0, 2),
        maps_tail.transpose(1, 0, 2),
    )


def local(size, *arrays):
    tokens, w_value, w_maps, state, w_up = (arrays[i] for i in (0, 3, 4, 14, 17))
    heads = state.shape[1]
    fits = (
        size in (2, 4, 8)
        and heads % GROUP == 0
        and state.shape[2:] == (HEAD_DIM, STATE)
        and w_maps.shape[1] == heads * 2 * STATE
        and all(extent % TILE == 0 for extent in (w_value.shape[1], w_maps.shape[1], w_up.shape[1], tokens.shape[1] * size))
        and tokens.shape[1] % LANES == 0
        and tokens.shape[0] % 8 == 0
    )
    return local_few(size, *arrays) if fits else local_many(*arrays)


def solution(mesh):
    in_specs = (
        P(("dp", "tp"), "kv"),
        P(),
        P(None, "kv"),
        P(None, "kv"),
        P(None, "kv"),
        P(),
        P(None, "kv"),
        P(None, "kv"),
        P(("dp", "tp"), None, "kv"),
        P(("dp", "tp"), None, "kv"),
        P("kv"),
        P("kv"),
        P("kv"),
        P("kv"),
        P(("dp", "tp"), "kv", None, None),
        P("kv", None),
        P(),
        P(None, "kv"),
        P("kv", None),
    )
    out_specs = (
        P(("dp", "tp"), "kv"),
        P(("dp", "tp"), "kv", None, None),
        P(("dp", "tp"), None, "kv"),
        P(("dp", "tp"), None, "kv"),
    )
    step = functools.partial(local, mesh.shape["kv"])
    return jax.shard_map(step, mesh=mesh, in_specs=in_specs, out_specs=out_specs, check_vma=False)
```

```python
import functools

import jax
import jax.numpy as jnp
from jax import lax
from jax.experimental import pallas as pl
from jax.experimental.pallas import tpu as pltpu
from jax.sharding import PartitionSpec as P

HEAD_DIM = 64
STATE = 128
LANES = 128
TILE = 1024
SLOTS = 3
LATE = 3
GROUP = 4


NORM_EPS = 1e-05

VMEM = pl.BlockSpec(memory_space=pltpu.VMEM)
HBM = pl.BlockSpec(memory_space=pltpu.HBM)


def rms_rows(matrix, gain_vec):
    widened = matrix.astype(jnp.float32)
    inv_scale = lax.rsqrt(jnp.mean(widened * widened, axis=-1, keepdims=True) + NORM_EPS)
    return (widened * inv_scale * gain_vec).astype(jnp.bfloat16)


def short_conv(past_rows, newest, kernel):
    window = jnp.concatenate([past_rows, newest[:, None, :]], axis=1)
    summed = jnp.sum(window.astype(jnp.float32) * kernel[None], axis=1)
    return (jax.nn.silu(summed), window[:, 1:, :])


def local_many(
    tokens,
    mix_gain,
    w_gate,
    w_value,
    w_maps,
    w_step,
    conv_value,
    conv_maps,
    past_value,
    past_maps,
    step_bias,
    decay_log,
    skip_gain,
    head_gain,
    state,
    w_out,
    mlp_gain,
    w_up,
    w_down,
):
    whole_rows = lax.all_gather(tokens, "kv", axis=1, tiled=True)
    batch_rows = whole_rows.shape[0]
    heads_here = state.shape[1]
    head_start = lax.axis_index("kv") * heads_here
    normed = rms_rows(whole_rows, mix_gain)
    gate_pre = jnp.dot(normed, w_gate, preferred_element_type=jnp.float32)
    step_cols = lax.dynamic_slice_in_dim(w_step, head_start, heads_here, 1)
    step_pre = jnp.dot(normed, step_cols, preferred_element_type=jnp.float32)
    value_new = jnp.dot(normed, w_value, preferred_element_type=jnp.float32).astype(jnp.bfloat16)
    maps_new = jnp.dot(normed, w_maps, preferred_element_type=jnp.float32).astype(jnp.bfloat16)
    value_act, value_tail = short_conv(past_value, value_new, conv_value)
    maps_act, maps_tail = short_conv(past_maps, maps_new, conv_maps)
    maps_act = lax.optimization_barrier(maps_act.astype(jnp.bfloat16))
    grouped = maps_act.astype(jnp.float32).reshape(batch_rows, -1, 2, STATE)
    per_group = heads_here // grouped.shape[1]
    in_map = jnp.repeat(grouped[:, :, 0], per_group, axis=1)
    out_map = jnp.repeat(grouped[:, :, 1], per_group, axis=1)
    head_values = value_act.reshape(batch_rows, heads_here, HEAD_DIM)
    step_size = jax.nn.softplus(step_pre + step_bias)
    decay_rate = jnp.exp(-step_size * jnp.exp(decay_log))
    written = (step_size[:, :, None] * head_values)[:, :, :, None] * in_map[:, :, None, :]
    state_next = decay_rate[:, :, None, None] * state + written
    read_out = (
        jnp.sum(state_next * out_map[:, :, None, :], axis=-1)
        + skip_gain[None, :, None] * head_values
    )
    gated_heads = read_out * jax.nn.silu(gate_pre.reshape(batch_rows, heads_here, HEAD_DIM))
    inv_scale = lax.rsqrt(jnp.mean(gated_heads * gated_heads, axis=-1, keepdims=True) + NORM_EPS)
    heads_out = gated_heads * inv_scale * head_gain.reshape(heads_here, HEAD_DIM)
    heads_out = heads_out.reshape(batch_rows, heads_here * HEAD_DIM).astype(jnp.bfloat16)
    partial_value = jnp.dot(heads_out, w_out, preferred_element_type=jnp.float32)
    own_part = lax.psum_scatter(partial_value, "kv", scatter_dimension=1, tiled=True)
    own_hidden = lax.optimization_barrier(
        (tokens.astype(jnp.float32) + own_part).astype(jnp.bfloat16)
    )
    hidden = lax.all_gather(own_hidden, "kv", axis=1, tiled=True)
    normed_mlp = rms_rows(hidden, mlp_gain)
    squared = jnp.square(jax.nn.relu(jnp.dot(normed_mlp, w_up, preferred_element_type=jnp.float32)))
    squared = squared.astype(jnp.bfloat16)
    partial_mlp = jnp.dot(squared, w_down, preferred_element_type=jnp.float32)
    mlp_part = lax.psum_scatter(partial_mlp, "kv", scatter_dimension=1, tiled=True)
    layer_out = (own_hidden.astype(jnp.float32) + mlp_part).astype(jnp.bfloat16)
    return (layer_out, state_next, value_tail, maps_tail)


def swapped(block, size, step):
    return lax.ppermute(block, "kv", [(i, i ^ step) for i in range(size)])


def shifted(block, size, step):
    return lax.ppermute(block, "kv", [(i, (i + step) % size) for i in range(size)])


def in_hbm(array):
    return pltpu.with_memory_space_constraint(array, pltpu.HBM)


def cost(flops, moved):
    return pl.CostEstimate(flops=int(flops), bytes_accessed=int(moved), transcendentals=0)


def silu(x):
    return x / (1.0 + jnp.exp(-x))


def row_copies(source, target, sems, first, parts):
    depth = source.shape[0] // parts
    blocks = [pl.ds(part * depth, depth) for part in range(parts)]
    return [
        pltpu.make_async_copy(source.at[block], target.at[block], sems.at[first + part])
        for part, block in enumerate(blocks)
    ]


def fetch_kernel(parts, *refs):
    count = len(parts)
    sources, targets, sems = refs[:count], refs[count:-1], refs[-1]
    copies = []
    for source, target, number in zip(sources, targets, parts):
        copies += row_copies(source, target, sems, len(copies), number)
    for copy in copies:
        copy.start()
    for copy in copies:
        copy.wait()


def fetch(arrays, parts, name):
    moved = sum(a.size * a.dtype.itemsize for a in arrays)
    return pl.pallas_call(
        functools.partial(fetch_kernel, parts),
        out_shape=[pltpu.VMEM(a.shape, a.dtype) for a in arrays],
        in_specs=[HBM] * len(arrays),
        out_specs=[VMEM] * len(arrays),
        scratch_shapes=[pltpu.SemaphoreType.DMA((sum(parts),))],
        compiler_params=pltpu.CompilerParams(vmem_limit_bytes=1 << 20),
        cost_estimate=cost(1e6, 2 * moved),
        name=name,
    )(*[in_hbm(a) for a in arrays])


def mixer_kernel(size, *refs):
    bias_ref, dlog_ref, skip_ref = refs[:3]
    refs = refs[3:]
    chunks = refs[:size]
    (gain, wstep, conv_v, conv_m, hgain, wmaps, pastv_s, pastm_s, wvalue, wgate, state, wout) = refs[
        size : 12 + size
    ]
    (part_o, x_o, state_o, dec_o, in_o, u_o, vtail, mtail) = refs[12 + size : 20 + size]
    (normed_s, wboth_s, raw_s, wout_s, newv_s, newm_s, out_s, value_s, gate_s, heads_s, sems, ssems) = refs[
        20 + size :
    ]
    rows, width = chunks[0].shape
    me = lax.axis_index("kv")
    heads = state.shape[1]
    pairs = heads // 2

    def state_copy(pair):
        both = pl.ds(2 * pair, 2)
        return pltpu.make_async_copy(state.at[:, both], state_o.at[:, both], ssems.at[pair])

    inner = wvalue.shape[1]
    load_value = row_copies(wvalue, wboth_s.at[:, pl.ds(0, inner)], sems, 0, 2)
    load_gate = row_copies(wgate, wboth_s.at[:, pl.ds(inner, inner)], sems, 2, 2)
    load_out = row_copies(wout, wout_s, sems, 4, 2)
    later = pairs - 2
    tails = [
        pltpu.make_async_copy(pastm_s.at[pl.ds(1, 2)], mtail.at[pl.ds(0, 2)], sems.at[6]),
        pltpu.make_async_copy(pastv_s.at[pl.ds(1, 2)], vtail.at[pl.ds(0, 2)], sems.at[7]),
        pltpu.make_async_copy(newm_s, mtail.at[2], sems.at[8]),
        pltpu.make_async_copy(newv_s, vtail.at[2], sems.at[9]),
    ]

    for copy in load_value + load_gate:
        copy.start()

    for step in range(size):
        source = lax.bitwise_xor(me, step)
        x_o[:, pl.ds(pl.multiple_of(source * width, width), width)] = chunks[step][...]
    x = x_o[...].astype(jnp.float32)
    inv = lax.rsqrt(jnp.mean(x * x, axis=-1, keepdims=True) + NORM_EPS)
    normed = (x * inv * gain[...]).astype(jnp.bfloat16)
    normed_s[...] = normed

    step_pre = lax.dot_general(
        normed, wstep[...], (((1,), (1,)), ((), ())), preferred_element_type=jnp.float32
    )

    def conv(past, new, taps, block):
        total = new.astype(jnp.float32) * taps[3:4, block]
        for t in range(3):
            total = total + past[t, :, block].astype(jnp.float32) * taps[t : t + 1, block]
        return silu(total)

    def span(index, extent):
        return pl.ds(pl.multiple_of(index * extent, extent), extent)

    def product(weights, block):
        return jnp.dot(normed_s[...], weights[:, block], preferred_element_type=jnp.float32)

    def maps_conv(tile):
        block = span(tile, TILE)
        act = conv(pastm_s, newm_s[:, block], conv_m, block).astype(jnp.bfloat16).astype(jnp.float32)
        groups = TILE // (2 * STATE)
        for group in range(groups):
            base = group * 2 * STATE
            target = span(tile * groups + group, STATE)
            in_o[:, target] = act[:, base : base + STATE]
            out_s[:, target] = act[:, base + STATE : base + 2 * STATE]

    def maps_body(tile, carry):
        @pl.when(tile < later)
        def _():
            state_copy(tile).start()

        maps_conv(jnp.maximum(tile - 1, 0))
        block = span(tile, TILE)
        newm_s[:, block] = product(wmaps, block).astype(jnp.bfloat16)
        return carry

    tiles = wmaps.shape[1] // TILE
    newm_s[:, :TILE] = jnp.zeros((rows, TILE), jnp.bfloat16)
    lax.fori_loop(0, tiles, maps_body, 0)
    for pair in range(tiles, later):
        state_copy(pair).start()
    for copy in load_value + load_gate:
        copy.wait()

    def raw_body(tile, carry):
        block = span(tile, TILE)
        raw_s[:, block] = product(wboth_s, block)
        return carry

    maps_conv(tiles - 1)
    lax.fori_loop(0, 2 * inner // TILE, raw_body, 0)

    def value_body(tile, carry):
        block = span(tile, TILE)
        new = raw_s[:, block].astype(jnp.bfloat16)
        newv_s[:, block] = new
        value_s[:, block] = conv(pastv_s, new, conv_v, block)
        gate_s[:, block] = silu(raw_s[:, span(tile + inner // TILE, TILE)])
        return carry

    lax.fori_loop(0, inner // TILE, value_body, 0)
    for copy in tails:
        copy.start()

    row_of = lax.broadcasted_iota(jnp.int32, (rows, STATE), 0)
    part_of = lax.broadcasted_iota(jnp.int32, (rows, GROUP * HEAD_DIM), 1) // HEAD_DIM
    low = lax.broadcasted_iota(jnp.int32, (rows, LANES), 1) < HEAD_DIM
    step_lane = lax.broadcasted_iota(jnp.int32, step_pre.shape, 1)
    head_lane = lax.broadcasted_iota(jnp.int32, (1, heads), 1)

    def of_head(ref, head):
        return jnp.sum(jnp.where(head_lane == head, ref[...], 0.0), axis=1, keepdims=True)

    def carried_sums(group, outs):
        total = None
        for row in range(0, rows, 2):
            wanted = [
                jnp.concatenate([jnp.where(row_of == row + t, out, 0.0) for t in range(2)], axis=1)
                for out in outs
            ]
            held = [
                state_o[row + t, pl.ds(group * GROUP, GROUP)].reshape(GROUP * HEAD_DIM, STATE)
                for t in range(2)
            ]
            term = lax.dot_general(
                jnp.concatenate(wanted, axis=0).astype(jnp.bfloat16),
                jnp.concatenate(held, axis=1).astype(jnp.bfloat16),
                (((1,), (1,)), ((), ())),
                preferred_element_type=jnp.float32,
            )
            total = term if total is None else total + term
        picked = None
        for which in range(GROUP):
            piece = jnp.where(part_of == which, total[which * rows : (which + 1) * rows], 0.0)
            picked = piece if picked is None else picked + piece
        return picked

    def group_body(group, carry):
        for which in range(GROUP // 2):
            pair = group * (GROUP // 2) + which
            state_copy(pair).wait()

            @pl.when(pair + later < pairs)
            def _():
                state_copy(pair + later).start()

            for part in range(2):

                @pl.when(pair == pairs - later + part)
                def _():
                    load_out[part].start()

        outs, decays, sizes, meets = [], [], [], []
        for which in range(GROUP):
            head = group * GROUP + which
            wide = span(head, STATE)
            column = jnp.sum(
                jnp.where(step_lane == me * heads + head, step_pre, 0.0), axis=1, keepdims=True
            )
            pre = jnp.broadcast_to(column, (rows, LANES)) + of_head(bias_ref, head)
            size_h = jnp.maximum(pre, 0.0) + jnp.log1p(jnp.exp(-jnp.abs(pre)))
            rate = jnp.exp(of_head(dlog_ref, head))
            decay = jnp.exp(-size_h * rate)
            dec_o[:, wide] = decay
            outs.append(out_s[:, wide])
            meets.append(jnp.sum(in_o[:, wide] * outs[-1], axis=1, keepdims=True))
            decays.append(decay)
            sizes.append(size_h)
        carried = carried_sums(group, outs)
        for which in range(GROUP // 2):
            one, two = 2 * which, 2 * which + 1
            block = span(group * (GROUP // 2) + which, LANES)
            value = value_s[:, block]
            written = jnp.where(low, sizes[one], sizes[two]) * value
            u_o[:, block] = written
            read = jnp.where(low, decays[one], decays[two]) * carried[:, which * LANES : (which + 1) * LANES]
            read = read + jnp.where(low, meets[one], meets[two]) * written
            skip = jnp.where(low, of_head(skip_ref, group * GROUP + one), of_head(skip_ref, group * GROUP + two))
            gated = (read + skip * value) * gate_s[:, block]
            square = gated * gated
            first = jnp.sum(jnp.where(low, square, 0.0), axis=1, keepdims=True)
            second = jnp.sum(jnp.where(low, 0.0, square), axis=1, keepdims=True)
            scale = lax.rsqrt(jnp.where(low, first, second) * (1.0 / HEAD_DIM) + NORM_EPS)
            heads_s[:, block] = (gated * scale * hgain[:, block]).astype(jnp.bfloat16)
        return carry

    lax.fori_loop(0, heads // GROUP, group_body, 0)

    half = inner // 2
    load_out[0].wait()

    def first_body(tile, carry):
        block = span(tile, TILE)
        raw_s[:, block] = jnp.dot(heads_s[:, :half], wout_s[:half, block], preferred_element_type=jnp.float32)
        return carry

    def second_body(tile, carry):
        block = span(tile, TILE)
        rest = jnp.dot(heads_s[:, half:], wout_s[half:, block], preferred_element_type=jnp.float32)
        part_o[:, block] = (raw_s[:, block] + rest).astype(jnp.bfloat16)
        return carry

    lax.fori_loop(0, wout_s.shape[1] // TILE, first_body, 0)
    load_out[1].wait()
    lax.fori_loop(0, wout_s.shape[1] // TILE, second_body, 0)
    for copy in tails:
        copy.wait()


def write_pairs(first, last, state_ref, dec_ref, in_ref, u_ref, next_ref, buffers, sems):
    rows = state_ref.shape[0]
    slots = buffers.shape[0]

    def store(pair, which):
        slot = lax.rem(pair, slots)
        return pltpu.make_async_copy(
            buffers.at[slot, which], next_ref.at[:, 2 * pair + which], sems.at[slot, which]
        )

    def pair_body(pair, carry):
        slot = lax.rem(pair, slots)
        turned = jnp.transpose(u_ref[:, pl.ds(pl.multiple_of(pair * LANES, LANES), LANES)])
        for which in range(2):

            @pl.when(pair >= first + slots)
            def _():
                store(pair - slots, which).wait()

            head = 2 * pair + which
            wide = pl.ds(pl.multiple_of(head * STATE, STATE), STATE)
            column = turned[which * HEAD_DIM : (which + 1) * HEAD_DIM]
            decay, in_map = dec_ref[:, wide], in_ref[:, wide]
            for row in range(rows):
                buffers[slot, which, row] = (
                    state_ref[row, head] * decay[row : row + 1]
                    + column[:, row : row + 1] * in_map[row : row + 1]
                )
            store(pair, which).start()
        return carry

    lax.fori_loop(first, last, pair_body, 0)
    for pair in range(max(last - slots, first), last):
        for which in range(2):
            store(pair, which).wait()


def early_kernel(first, last, parts, *refs):
    wup, next_ref, wup_o, buffers, sems, wsems = refs[4:]
    loads = row_copies(wup, wup_o, wsems, 0, parts)
    for copy in loads:
        copy.start()
    write_pairs(first, last, *refs[:4], next_ref, buffers, sems)
    for copy in loads:
        copy.wait()


def late_kernel(first, last, *refs):
    next_ref, buffers, sems = refs[5:]
    write_pairs(first, last, *refs[:4], next_ref, buffers, sems)


def mlp_kernel(size, *refs):
    x_ref = refs[0]
    parts = refs[1 : 1 + size]
    gain, wup, wdown = refs[1 + size : 4 + size]
    base_o = refs[4 + size]
    pieces = refs[5 + size : 4 + 2 * size]
    hidden_s, total_s, normed_s, squared_s, wdown_s, sems = refs[4 + 2 * size :]
    loads = row_copies(wdown, wdown_s, sems, 0, sems.shape[0])
    for copy in loads:
        copy.start()
    width = base_o.shape[1]
    me = lax.axis_index("kv")
    total = x_ref[...].astype(jnp.float32)
    for part in parts:
        total = total + part[...].astype(jnp.float32)
    hidden = total.astype(jnp.bfloat16)
    hidden_s[...] = hidden.astype(jnp.float32)
    wide = hidden_s[...]
    inv = lax.rsqrt(jnp.mean(wide * wide, axis=-1, keepdims=True) + NORM_EPS)
    normed = (wide * inv * gain[...]).astype(jnp.bfloat16)
    normed_s[...] = normed

    def up_body(tile, carry):
        block = pl.ds(pl.multiple_of(tile * TILE, TILE), TILE)
        up = jnp.maximum(jnp.dot(normed_s[...], wup[:, block], preferred_element_type=jnp.float32), 0.0)
        squared_s[:, block] = (up * up).astype(jnp.bfloat16)
        return carry

    lax.fori_loop(0, wup.shape[1] // TILE, up_body, 0)
    depth = wdown.shape[0] // sems.shape[0]
    total_s[...] = jnp.zeros(total_s.shape, jnp.float32)

    def down_body(part, carry):
        block = pl.ds(pl.multiple_of(part * depth, depth), depth)
        pltpu.make_async_copy(wdown.at[block], wdown_s.at[block], sems.at[part]).wait()
        total_s[...] += jnp.dot(squared_s[:, block], wdown_s[block, :], preferred_element_type=jnp.float32)
        return carry

    lax.fori_loop(0, sems.shape[0], down_body, 0)
    own = pl.ds(pl.multiple_of(me * width, width), width)
    base_o[...] = hidden_s[:, own] + total_s[:, own]
    for step in range(1, size):
        target = lax.rem(me + step, size)
        block = pl.ds(pl.multiple_of(target * width, width), width)
        pieces[step - 1][...] = total_s[:, block].astype(jnp.bfloat16)


def local_few(
    size,
    tokens,
    mix_gain,
    w_gate,
    w_value,
    w_maps,
    w_step,
    conv_value,
    conv_maps,
    past_value,
    past_maps,
    step_bias,
    decay_log,
    skip_gain,
    head_gain,
    state,
    w_out,
    mlp_gain,
    w_up,
    w_down,
):
    f32, bf16 = jnp.float32, jnp.bfloat16
    rows, width = tokens.shape
    model = width * size
    heads = state.shape[1]
    inner, maps = w_value.shape[1], w_maps.shape[1]

    chunks = [tokens] + [swapped(tokens, size, step) for step in range(1, size)]
    past_value, past_maps = past_value.transpose(1, 0, 2), past_maps.transpose(1, 0, 2)
    maps_near, value_near, past_near = fetch([w_maps, past_value, past_maps], (8, 1, 1), "fetch_maps")
    part, whole, held, decay, in_map, written, value_tail, maps_tail = pl.pallas_call(
        functools.partial(mixer_kernel, size),
        out_shape=[
            pltpu.VMEM((rows, model), bf16),
            pltpu.VMEM((rows, model), bf16),
            pltpu.VMEM(state.shape, f32),
            pltpu.VMEM((rows, heads * STATE), f32),
            pltpu.VMEM((rows, heads * STATE), f32),
            pltpu.VMEM((rows, inner), f32),
            jax.ShapeDtypeStruct((3, rows, inner), bf16),
            jax.ShapeDtypeStruct((3, rows, maps), bf16),
        ],
        in_specs=[VMEM] * (size + 11) + [HBM] * 4,
        out_specs=[VMEM] * 6 + [HBM] * 2,
        scratch_shapes=[
            pltpu.VMEM((rows, model), bf16),
            pltpu.VMEM((model, 2 * inner), bf16),
            pltpu.VMEM((rows, max(2 * inner, model)), f32),
            pltpu.VMEM(w_out.shape, bf16),
            pltpu.VMEM((rows, inner), bf16),
            pltpu.VMEM((rows, maps), bf16),
            pltpu.VMEM((rows, heads * STATE), f32),
            pltpu.VMEM((rows, inner), f32),
            pltpu.VMEM((rows, inner), f32),
            pltpu.VMEM((rows, inner), bf16),
            pltpu.SemaphoreType.DMA((10,)),
            pltpu.SemaphoreType.DMA((heads // 2,)),
        ],
        compiler_params=pltpu.CompilerParams(vmem_limit_bytes=20 << 20),
        cost_estimate=cost(2 * rows * model * (2 * inner + maps), 40e6),
        name="mixer",
    )(
        step_bias.reshape(1, -1),
        decay_log.reshape(1, -1),
        skip_gain.reshape(1, -1),
        *chunks,
        mix_gain.reshape(1, -1),
        w_step.T,
        conv_value,
        conv_maps,
        head_gain.reshape(1, -1),
        maps_near,
        value_near,
        past_near,
        *[in_hbm(a) for a in (w_value, w_gate, state, w_out)],
    )

    parts = [part] + [shifted(part, size, step) for step in range(1, size)]
    pairs = heads // 2
    middle = pairs - pairs * LATE // 8
    state_first, up_near = pl.pallas_call(
        functools.partial(early_kernel, 0, middle, 4),
        out_shape=[jax.ShapeDtypeStruct(state.shape, f32), pltpu.VMEM(w_up.shape, bf16)],
        in_specs=[VMEM] * 4 + [HBM],
        out_specs=[HBM, VMEM],
        scratch_shapes=[
            pltpu.VMEM((SLOTS, 2, rows, HEAD_DIM, STATE), f32),
            pltpu.SemaphoreType.DMA((SLOTS, 2)),
            pltpu.SemaphoreType.DMA((4,)),
        ],
        compiler_params=pltpu.CompilerParams(vmem_limit_bytes=8 << 20),
        cost_estimate=cost(1e6, 33e6),
        name="write_early",
    )(held, decay, in_map, written, in_hbm(w_up))
    base, *pieces = pl.pallas_call(
        functools.partial(mlp_kernel, size),
        out_shape=[pltpu.VMEM((rows, width), f32)] + [pltpu.VMEM((rows, width), bf16)] * (size - 1),
        in_specs=[VMEM] * (size + 3) + [HBM],
        out_specs=[VMEM] * size,
        scratch_shapes=[
            pltpu.VMEM((rows, model), f32),
            pltpu.VMEM((rows, model), f32),
            pltpu.VMEM((rows, model), bf16),
            pltpu.VMEM((rows, w_up.shape[1]), bf16),
            pltpu.VMEM(w_down.shape, bf16),
            pltpu.SemaphoreType.DMA((4,)),
        ],
        compiler_params=pltpu.CompilerParams(vmem_limit_bytes=12 << 20),
        cost_estimate=cost(4 * rows * model * w_up.shape[1], 17e6),
        name="mlp",
    )(whole, *parts, mlp_gain.reshape(1, -1), up_near, in_hbm(w_down))

    arrived = [shifted(pieces[step - 1], size, step) for step in range(size - 1, 0, -1)]
    held, decay, in_map, written, _ = lax.optimization_barrier((held, decay, in_map, written, base))
    state_next = pl.pallas_call(
        functools.partial(late_kernel, middle, pairs),
        out_shape=jax.ShapeDtypeStruct(state.shape, f32),
        in_specs=[VMEM] * 4 + [HBM],
        out_specs=HBM,
        scratch_shapes=[
            pltpu.VMEM((SLOTS, 2, rows, HEAD_DIM, STATE), f32),
            pltpu.SemaphoreType.DMA((SLOTS, 2)),
        ],
        input_output_aliases={4: 0},
        compiler_params=pltpu.CompilerParams(vmem_limit_bytes=8 << 20),
        cost_estimate=cost(1e6, 1e7),
        name="write_late",
    )(held, decay, in_map, written, in_hbm(state_first))
    total = base
    for piece in arrived:
        total = total + piece.astype(f32)
    return (
        total.astype(bf16),
        state_next,
        value_tail.transpose(1, 0, 2),
        maps_tail.transpose(1, 0, 2),
    )


def local(size, *arrays):
    tokens, w_value, w_maps, state, w_up = (arrays[i] for i in (0, 3, 4, 14, 17))
    heads = state.shape[1]
    fits = (
        size in (2, 4, 8)
        and heads % GROUP == 0
        and state.shape[2:] == (HEAD_DIM, STATE)
        and w_maps.shape[1] == heads * 2 * STATE
        and all(extent % TILE == 0 for extent in (w_value.shape[1], w_maps.shape[1], w_up.shape[1], tokens.shape[1] * size))
        and tokens.shape[1] % LANES == 0
        and tokens.shape[0] % 8 == 0
    )
    return local_few(size, *arrays) if fits else local_many(*arrays)


def solution(mesh):
    in_specs = (
        P(("dp", "tp"), "kv"),
        P(),
        P(None, "kv"),
        P(None, "kv"),
        P(None, "kv"),
        P(),
        P(None, "kv"),
        P(None, "kv"),
        P(("dp", "tp"), None, "kv"),
        P(("dp", "tp"), None, "kv"),
        P("kv"),
        P("kv"),
        P("kv"),
        P("kv"),
        P(("dp", "tp"), "kv", None, None),
        P("kv", None),
        P(),
        P(None, "kv"),
        P("kv", None),
    )
    out_specs = (
        P(("dp", "tp"), "kv"),
        P(("dp", "tp"), "kv", None, None),
        P(("dp", "tp"), None, "kv"),
        P(("dp", "tp"), None, "kv"),
    )
    step = functools.partial(local, mesh.shape["kv"])
    return jax.shard_map(step, mesh=mesh, in_specs=in_specs, out_specs=out_specs, check_vma=False)
```
